512 devices in a mesh: sp: 64 (over z, y), tp: 8 (over x, core).
Axes of the slice: x: 4, y: 8, z: 8, core: 2. Of those that a mesh axis runs over, the one named last changes fastest.
Arguments:
- layer_source_tokens: bfloat16 [2, 4096, 4096], P(None, 'sp'), may hold values from -6 to 6
- address_projection: bfloat16 [4096, 2048], P('sp', 'tp'), may hold values from -0.09375 to 0.09375
- content_projection: bfloat16 [4096, 2048], P('sp', 'tp'), may hold values from -0.09375 to 0.09375
- strength_projection: bfloat16 [4096, 16], replicated, may hold values from -0.09375 to 0.09375
- fading_driver_projection: bfloat16 [4096, 16], replicated, may hold values from -0.25 to 0.25
- strength_offset: float32 [16], P('tp'), may hold values from -2.5 to 1
- channel_fading_speed: float32 [16], P('tp')
- added_fading_exponent: float32 [2, 4096, 16], P(None, 'sp', 'tp'), may hold values from -0.7 to 0, as said below
- first_step_probe: bfloat16 [2, 2048], P(None, 'tp'), may hold values from -6 to 6
- first_step_address: bfloat16 [2, 2048], P(None, 'tp'), may hold values from -6 to 6
- first_step_content: bfloat16 [2, 2048], P(None, 'tp'), may hold values from -6 to 6
- first_step_outgate: bfloat16 [2, 2048], P(None, 'tp'), may hold values from -6 to 6
- first_step_strength_raw: float32 [2, 16], P(None, 'tp'), may hold values from -6 to 6
- channel_scaling_factor: float32 [128], replicated, may hold values from 0.1 to 1.9
- readout_projection: bfloat16 [2048, 4096], P('tp', 'sp'), may hold values from -0.125 to 0.125
Outputs:
- state_cache: bfloat16 [2, 16, 128, 128], P(None, 'tp')
- mixed_read: bfloat16 [2, 4096], P(None, 'sp')
- boundary_cache: bfloat16 [2, 64, 16, 128, 128], P(None, 'sp', 'tp')
The draws below stay inside these ranges and needn't reach their ends.
Inputs may be any that keep to these rules, and one draw needn't show every extreme that they name: `added_fading_exponent`: zero at most positions.
All inputs are finite; a program needn't handle non-finite values.
Results may differ from the reference program's by a relative error of at most 0.017.
Values may be sent and summed in bfloat16 or wider, within the bound.
No kernel may reach another device: no remote copies, remote signals or barrier semaphores. Data moves between devices by JAX's collectives and lax.ppermute only.
A program may use at most 64 MiB of HBM per device.

```python
import jax
import jax.numpy as jnp
from jax import lax

D = 4096
H = 16
ADDRESS_WIDTH = 128
BLOCK = 64
NSEQ = 2
LEN = 4096
RANGES = 64
N_TP = 8


def draw_channel_fading_speed(key, part):
    low_rate = 0.3 / LEN
    high_rate = 0.05
    uniform_draw = jax.random.uniform(jax.random.fold_in(key, 11), (H,), jnp.float32)
    return jnp.exp(jnp.log(low_rate) + uniform_draw * (jnp.log(high_rate) - jnp.log(low_rate)))


def draw_added_fading_exponent(key, part):
    chosen = jax.random.uniform(jax.random.fold_in(key, 21), (NSEQ, LEN, H), jnp.float32)
    kept_share = jax.random.uniform(jax.random.fold_in(key, 22), (NSEQ, LEN, H), jnp.float32, 0.5, 0.8)
    return jnp.where(chosen < 3.0 / LEN, jnp.log(kept_share), 0.0)


def block_levels(rng, shape, shards, low, top_value):
    factor_of = 1.0
    for position, shards_of in shards:
        steps = jax.random.uniform(jax.random.fold_in(jax.random.fold_in(rng, 6), position), (shards_of,), jnp.float32, low / len(shards), top_value / len(shards))
        factor_of = factor_of * jnp.repeat(jnp.exp(steps), shape[position] // shards_of).reshape((-1,) + (1,) * (len(shape) - 1 - position))
    return factor_of


def centred(own_key, dims, width, most, shards=(), kind=jnp.bfloat16):
    drawn = width * jax.random.normal(own_key, dims, jnp.float32)
    if shards:
        drawn = drawn * block_levels(own_key, dims, shards, -0.22, 0.18)
    return jnp.clip(drawn, -most, most).astype(kind)


def setup_inputs(seed: int = 0) -> dict:
    key_list = jax.random.split(jax.random.key(seed), 16)
    layer_source_tokens = centred(key_list[0], (NSEQ, LEN, D), 1.0, 6.0, ((1, 64),))
    address_projection = centred(key_list[1], (D, H * ADDRESS_WIDTH), D ** -0.5, 0.09375, ((0, 64), (1, 8)))
    content_projection = centred(key_list[2], (D, H * ADDRESS_WIDTH), D ** -0.5, 0.09375, ((0, 64), (1, 8)))
    strength_projection = centred(key_list[3], (D, H), D ** -0.5, 0.09375)
    fading_driver_projection = centred(key_list[4], (D, H), (D // 9) ** -0.5, 0.25)
    strength_offset = jnp.clip(-2.5 + 3.5 * jax.random.uniform(key_list[5], (H,), jnp.float32) ** block_levels(key_list[5], (H,), ((0, 8),), -0.2, 0.2), -2.5, 1.0)
    channel_fading_speed = draw_channel_fading_speed(jax.random.fold_in(key_list[15], 71), 0)
    added_fading_exponent = draw_added_fading_exponent(jax.random.fold_in(key_list[15], 71), 0)
    first_step_probe = centred(key_list[8], (NSEQ, H * ADDRESS_WIDTH), 1.0, 6.0, ((1, 8),))
    first_step_address = centred(key_list[9], (NSEQ, H * ADDRESS_WIDTH), 1.0, 6.0, ((1, 8),))
    first_step_content = centred(key_list[10], (NSEQ, H * ADDRESS_WIDTH), 1.0, 6.0, ((1, 8),))
    first_step_outgate = centred(key_list[11], (NSEQ, H * ADDRESS_WIDTH), 1.0, 6.0, ((1, 8),))
    first_step_strength_raw = centred(key_list[12], (NSEQ, H), 1.5, 6.0, ((1, 8),), jnp.float32)
    channel_scaling_factor = jnp.clip(1.0 + 0.18 * jax.random.normal(key_list[13], (ADDRESS_WIDTH,), jnp.float32), 0.1, 1.9)
    readout_projection = centred(key_list[14], (H * ADDRESS_WIDTH, D), (H * ADDRESS_WIDTH) ** -0.5, 0.125, ((0, 8), (1, 64)))
    return {"layer_source_tokens": layer_source_tokens, "address_projection": address_projection, "content_projection": content_projection, "strength_projection": strength_projection, "fading_driver_projection": fading_driver_projection, "strength_offset": strength_offset, "channel_fading_speed": channel_fading_speed, "added_fading_exponent": added_fading_exponent, "first_step_probe": first_step_probe, "first_step_address": first_step_address, "first_step_content": first_step_content, "first_step_outgate": first_step_outgate, "first_step_strength_raw": first_step_strength_raw, "channel_scaling_factor": channel_scaling_factor, "readout_projection": readout_projection}


EPSILON = 1e-06
HIGHEST_ACCURACY = lax.Precision.HIGHEST

def unit_inverse(lower_part):
    matrix_order = lower_part.shape[-1]
    identity = jnp.eye(matrix_order, dtype=jnp.float32)
    result = identity - lower_part
    power_term = lower_part
    reached = 2
    while reached < matrix_order:
        power_term = jnp.matmul(power_term, power_term, precision=HIGHEST_ACCURACY)
        result = jnp.matmul(result, identity + power_term, precision=HIGHEST_ACCURACY)
        reached = reached * 2
    return result

def build_arguments(address_vectors, content_vectors, outgate_raw_scores, strength_offset, channel_fading_speed, added_fading_exponent, channel_width):
    length = address_vectors.shape[0]
    attention_channels_total = channel_fading_speed.shape[0]
    address_token_slab = jax.nn.silu(address_vectors.astype(jnp.float32)).reshape(length, attention_channels_total, channel_width)
    address_token_slab = address_token_slab * lax.rsqrt(lax.optimization_barrier(jnp.sum(address_token_slab * address_token_slab, axis=-1, keepdims=True)) + EPSILON)
    content_token_slab = jax.nn.silu(content_vectors.astype(jnp.float32)).reshape(length, attention_channels_total, channel_width)
    strength_raw_expanded = outgate_raw_scores.astype(jnp.float32)
    storing_strength = jax.nn.sigmoid(strength_raw_expanded[:, :attention_channels_total] + strength_offset)
    fading_exponent = added_fading_exponent - channel_fading_speed * jax.nn.softplus(strength_raw_expanded[:, attention_channels_total:])
    return (address_token_slab, content_token_slab, storing_strength, fading_exponent)

def final_state(address_token_slab, content_token_slab, storing_strength, fading_exponent, block):
    length, attention_channels_total, channel_width = address_token_slab.shape
    blocks = length // block

    def split_blocks(tensor):
        moved_axes = jnp.swapaxes(tensor, 0, 1)
        return moved_axes.reshape((attention_channels_total, blocks, block) + moved_axes.shape[2:])
    block_keys = split_blocks(address_token_slab)
    block_values = split_blocks(content_token_slab)
    block_beta = split_blocks(storing_strength)
    cumulative = jnp.cumsum(split_blocks(fading_exponent), axis=-1)
    positions = jnp.arange(block)
    strict = positions[:, None] > positions[None, :]
    spread_log = jnp.where(strict, cumulative[..., :, None] - cumulative[..., None, :], 0.0)
    scaled_keys = block_keys * block_beta[..., None]
    inner_prod = jnp.einsum('hnik,hnjk->hnij', scaled_keys, block_keys, precision=HIGHEST_ACCURACY)
    lower_part = jnp.where(strict, inner_prod * jnp.exp(spread_log), 0.0)
    inverse = unit_inverse(lower_part)
    targets = jnp.concatenate([block_values * block_beta[..., None], scaled_keys * jnp.exp(cumulative)[..., None]], axis=-1)
    solved = jnp.einsum('hnij,hnjk->hnik', inverse, targets, precision=HIGHEST_ACCURACY)
    updates = solved[..., :channel_width]
    key_weights = solved[..., channel_width:]
    tail_keys = block_keys * jnp.exp(cumulative[..., -1:] - cumulative)[..., None]
    last_decay = jnp.exp(cumulative[..., -1])

    def advance(carried_state, block_items):
        update_index, weight_index, tail_index, last_index = block_items
        fresh_value_rows = update_index - jnp.einsum('xbg,xgp->xbp', weight_index, carried_state, precision=HIGHEST_ACCURACY)
        carried_state = carried_state * last_index[:, None, None] + jnp.einsum('tjo,tjw->tow', tail_index, fresh_value_rows, precision=HIGHEST_ACCURACY)
        return (carried_state, None)

    def range_advance(carried_state, range_items):
        carried_state, _ = lax.scan(advance, carried_state, range_items)
        return (carried_state, carried_state)
    blocks_per_range = blocks // RANGES
    initial = jnp.zeros((attention_channels_total, channel_width, channel_width), jnp.float32)
    block_items = (jnp.moveaxis(updates, 1, 0), jnp.moveaxis(key_weights, 1, 0), jnp.moveaxis(tail_keys, 1, 0), jnp.moveaxis(last_decay, 1, 0))
    range_items = tuple((item.reshape((RANGES, blocks_per_range) + item.shape[1:]) for item in block_items))
    _, range_states = lax.scan(range_advance, initial, range_items)
    return range_states

def read_heads(state_cache, first_step_probe, first_step_address, first_step_content, first_step_outgate, first_step_strength_raw, channel_scaling_factor):
    seq_count, attention_channels_total, channel_width, _ = state_cache.shape
    carried_state = state_cache.astype(jnp.float32)

    def activate(tensor):
        return jax.nn.silu(tensor.astype(jnp.float32)).reshape(seq_count, attention_channels_total, channel_width)
    query_rows = activate(first_step_probe)
    address_token_slab = activate(first_step_address)
    address_token_slab = address_token_slab * lax.rsqrt(lax.optimization_barrier(jnp.sum(address_token_slab * address_token_slab, axis=-1, keepdims=True)) + EPSILON)
    content_token_slab = activate(first_step_content)
    storing_strength = jax.nn.sigmoid(first_step_strength_raw)
    recalled = jnp.einsum('nhk,nhkv->nhv', address_token_slab, carried_state, precision=HIGHEST_ACCURACY)
    updated = carried_state + storing_strength[..., None, None] * address_token_slab[..., :, None] * (content_token_slab - recalled)[..., None, :]
    output = jnp.einsum('nhk,nhkv->nhv', query_rows, updated, precision=HIGHEST_ACCURACY)
    normed = output * lax.rsqrt(lax.optimization_barrier(jnp.mean(output * output, axis=-1, keepdims=True)) + EPSILON) * channel_scaling_factor
    gated_out = normed * activate(first_step_outgate)
    return gated_out.reshape(seq_count, attention_channels_total * channel_width).astype(jnp.bfloat16)

def reference(layer_source_tokens, address_projection, content_projection, strength_projection, fading_driver_projection, strength_offset, channel_fading_speed, added_fading_exponent, first_step_probe, first_step_address, first_step_content, first_step_outgate, first_step_strength_raw, channel_scaling_factor, readout_projection):
    seq_count, length, model_width = layer_source_tokens.shape
    flat_rows = layer_source_tokens.reshape(seq_count * length, model_width)

    def product(weight):
        return jnp.dot(flat_rows, weight, preferred_element_type=jnp.float32).astype(jnp.bfloat16)
    address_vectors = product(address_projection).reshape(seq_count, length, -1)
    content_vectors = product(content_projection).reshape(seq_count, length, -1)
    outgate_raw_scores = jnp.concatenate([product(strength_projection), product(fading_driver_projection)], axis=-1).reshape(seq_count, length, -1)

    def solitary_prompt(prompt_members):
        address_token_list, content_token_list, strength_raw_list, prompt_group_tokens = prompt_members
        address_token_slab, content_token_slab, storing_strength, fading_exponent = build_arguments(address_token_list, content_token_list, strength_raw_list, strength_offset, channel_fading_speed, prompt_group_tokens, ADDRESS_WIDTH)
        return final_state(address_token_slab, content_token_slab, storing_strength, fading_exponent, BLOCK)
    range_memories = lax.map(solitary_prompt, (address_vectors, content_vectors, outgate_raw_scores, added_fading_exponent))
    boundary_cache = range_memories.astype(jnp.bfloat16)
    state_cache = range_memories[:, -1].astype(jnp.bfloat16)
    heads_read = read_heads(state_cache, first_step_probe, first_step_address, first_step_content, first_step_outgate, first_step_strength_raw, channel_scaling_factor)
    group_rows = heads_read.astype(jnp.float32).reshape(seq_count, N_TP, -1)
    group_weights = readout_projection.astype(jnp.float32).reshape(N_TP, -1, model_width)
    group_terms = jnp.einsum('stc,tcd->tsd', group_rows, group_weights)
    rounded = lax.optimization_barrier(group_terms.astype(jnp.bfloat16))
    mixed_read = lax.optimization_barrier(jnp.sum(rounded.astype(jnp.float32), axis=0)).astype(jnp.bfloat16)
    return (state_cache, mixed_read, boundary_cache)
```

```python
import jax
import jax.numpy as jnp
from jax import lax
from jax.sharding import Mesh
from jax.sharding import PartitionSpec as P

WIDTH = 128
SIDE = 8
EPSILON = 1e-06
BEST = lax.Precision.HIGHEST
SP = ("z", "y")


def exchange(messages, axis):
    return lax.all_to_all(messages, axis, split_axis=0, concat_axis=0, tiled=True)


def from_everyone(array, axis):
    return exchange(jnp.broadcast_to(array, (lax.axis_size(axis), *array.shape)), axis)


def unit_inverse(lower_part):
    order = lower_part.shape[-1]
    identity = jnp.eye(order, dtype=jnp.float32)
    result = identity - lower_part
    power = lower_part
    reached = 2
    while reached < order:
        power = jnp.matmul(power, power, precision=BEST)
        result = jnp.matmul(result, identity + power, precision=BEST)
        reached *= 2
    return result


def two_parts(values):
    high = lax.reduce_precision(values, 8, 7)
    return high.astype(jnp.bfloat16), (values - high).astype(jnp.bfloat16)


def range_maps(keys, values, beta, fading):
    block = keys.shape[1]
    cumulative = jnp.cumsum(fading, axis=-1)
    at = jnp.arange(block)
    strict = at[:, None] > at[None, :]
    spread = jnp.where(strict, cumulative[:, :, None] - cumulative[:, None, :], 0.0)
    scaled = keys * beta[..., None]
    inner = jnp.einsum("nik,njk->nij", scaled, keys, precision=BEST)
    inverse = unit_inverse(jnp.where(strict, inner * jnp.exp(spread), 0.0))
    targets = jnp.concatenate(
        [scaled * jnp.exp(cumulative)[..., None], values * beta[..., None]], axis=-1
    )
    solved = jnp.einsum("nij,njk->nik", inverse, targets, precision=BEST)
    last = cumulative[:, -1:]
    tail = keys * jnp.exp(last - cumulative)[..., None]
    moved = jnp.einsum("njk,njw->nkw", tail, solved, precision=BEST)
    identity = jnp.eye(WIDTH, dtype=jnp.float32)
    transition = jnp.exp(last)[..., None] * identity - moved[..., :WIDTH]
    return jnp.concatenate([transition, moved[..., WIDTH:]], axis=-1)


def then(earlier, later):
    both = jnp.matmul(later[..., :WIDTH], earlier, precision=BEST)
    return jnp.concatenate([both[..., :WIDTH], both[..., WIDTH:] + later[..., WIDTH:]], axis=-1)


def applied(maps, state):
    return jnp.matmul(maps[..., :WIDTH], state, precision=BEST) + maps[..., WIDTH:]


def read_heads(state_cache, probe, address, content, outgate, strength_raw, gain):
    prompts, heads, width, _ = state_cache.shape
    state = state_cache.astype(jnp.float32)

    def activate(tensor):
        return jax.nn.silu(tensor.astype(jnp.float32)).reshape(prompts, heads, width)

    query = activate(probe)
    key = activate(address)
    key = key * lax.rsqrt(jnp.sum(key * key, axis=-1, keepdims=True) + EPSILON)
    value = activate(content)
    strength = jax.nn.sigmoid(strength_raw)
    recalled = jnp.einsum("nhk,nhkv->nhv", key, state, precision=BEST)
    updated = state + strength[..., None, None] * key[..., :, None] * (value - recalled)[..., None, :]
    output = jnp.einsum("nhk,nhkv->nhv", query, updated, precision=BEST)
    normed = output * lax.rsqrt(jnp.mean(output * output, axis=-1, keepdims=True) + EPSILON) * gain
    return (normed * activate(outgate)).reshape(prompts, heads * width).astype(jnp.bfloat16)


def per_device(
    tokens,
    address_projection,
    content_projection,
    strength_projection,
    fading_driver_projection,
    strength_offset,
    fading_speed,
    added_fading,
    probe,
    address,
    content,
    outgate,
    strength_raw,
    gain,
    readout_projection,
):
    prompts, positions, model = tokens.shape
    heads = fading_speed.shape[0]
    rows = prompts * positions
    share = model // (SIDE * SIDE)
    z, y, tp = lax.axis_index("z"), lax.axis_index("y"), lax.axis_index("tp")
    half = SIDE // 2
    my_half = y % 2

    weights = jnp.concatenate(
        [
            part[:, head * WIDTH : (head + 1) * WIDTH]
            for head in range(heads)
            for part in (address_projection, content_projection)
        ],
        axis=1,
    )
    flat = tokens.reshape(rows, model)
    columns = flat.reshape(rows, SIDE, SIDE, share).transpose(2, 0, 1, 3).reshape(SIDE, rows, -1)
    line_tokens = exchange(columns, "y")
    line_weights = from_everyone(weights, "z").reshape(SIDE * share, -1)

    drivers = jnp.concatenate([strength_projection, fading_driver_projection], axis=1)
    logits = jnp.dot(flat, drivers, preferred_element_type=jnp.float32).astype(jnp.bfloat16)
    logits = logits.astype(jnp.float32).reshape(prompts, positions, 2, -1)
    mine = lax.dynamic_slice_in_dim(logits, tp * heads, heads, 3)
    beta = jax.nn.sigmoid(mine[:, :, 0] + strength_offset)
    fading = added_fading - fading_speed * jax.nn.softplus(mine[:, :, 1])
    gates = jnp.stack([*two_parts(beta), *two_parts(fading)])
    gates = gates.transpose(1, 3, 0, 2).reshape(prompts, heads, 1, 1, 4 * positions)

    partial = jnp.dot(
        line_tokens.reshape(SIDE * rows, -1), line_weights, preferred_element_type=jnp.float32
    ).astype(jnp.bfloat16)
    partial = partial.reshape(2, half, prompts, positions, heads, 2 * WIDTH)
    partial = partial.transpose(2, 4, 0, 1, 3, 5).reshape(
        prompts, heads, 2, half * positions, 2 * WIDTH
    )
    gates = jnp.broadcast_to(gates, (prompts, heads, 2, 16, 4 * positions))
    sent = jnp.concatenate([partial, gates], axis=3).reshape(SIDE, half * positions + 16, -1)
    got = exchange(sent, "y")

    sums = got[:, : half * positions].astype(jnp.float32).sum(axis=0)
    sums = sums.reshape(half, positions, 2 * WIDTH)
    gates = lax.dynamic_slice_in_dim(got[:, half * positions], my_half * half, half, 0)
    gates = gates.astype(jnp.float32).reshape(half, 4, positions)
    beta = gates[:, 0] + gates[:, 1]
    fading = gates[:, 2] + gates[:, 3]
    keys = jax.nn.silu(sums[..., :WIDTH])
    keys = keys * lax.rsqrt(jnp.sum(keys * keys, axis=-1, keepdims=True) + EPSILON)
    values = jax.nn.silu(sums[..., WIDTH:])
    maps = range_maps(keys, values, beta, fading)
    inside = [maps[0]]
    for j in range(1, half):
        inside.append(then(inside[-1], maps[j]))

    whole = inside[-1].astype(jnp.bfloat16)
    other = lax.ppermute(whole, "y", [(i, i ^ 1) for i in range(SIDE)])
    first = jnp.where(my_half == 0, whole, other).astype(jnp.float32)
    second = jnp.where(my_half == 0, other, whole).astype(jnp.float32)
    line = then(first, second).astype(jnp.bfloat16)
    lines = from_everyone(line, "z").astype(jnp.float32)
    state = jnp.zeros((WIDTH, WIDTH), jnp.float32)
    entering = state
    for k in range(SIDE):
        entering = jnp.where(z == k, state, entering)
        state = applied(lines[k], state) if k else lines[0][:, WIDTH:]
    entering = jnp.where(my_half == 0, entering, applied(first, entering))
    leaving = applied(jnp.stack(inside), entering).astype(jnp.bfloat16)

    final_half = lax.dynamic_slice_in_dim(
        state.astype(jnp.bfloat16), my_half * (WIDTH // 2), WIDTH // 2, 0
    )
    home = jnp.concatenate(
        [
            jnp.concatenate([leaving, leaving], axis=0),
            jnp.broadcast_to(final_half, (SIDE, *final_half.shape)),
        ],
        axis=1,
    )
    back = exchange(home, "y").reshape(prompts, heads, 2, WIDTH + WIDTH // 2, WIDTH)
    boundary = lax.dynamic_index_in_dim(back, y // half, 2, keepdims=False)[:, :, :WIDTH]
    state_cache = back[:, :, :, WIDTH:].reshape(prompts, heads, WIDTH, WIDTH)

    heads_read = read_heads(state_cache, probe, address, content, outgate, strength_raw, gain)
    terms = jnp.dot(heads_read, readout_projection, preferred_element_type=jnp.float32)
    mixed = from_everyone(terms.astype(jnp.bfloat16), "tp").astype(jnp.float32).sum(axis=0)
    return state_cache, mixed.astype(jnp.bfloat16), boundary[:, None]


def solution(mesh):
    finer = Mesh(mesh.devices.reshape(SIDE, SIDE, mesh.shape["tp"]), (*SP, "tp"))
    return jax.shard_map(
        per_device,
        mesh=finer,
        in_specs=(
            P(None, SP, None),
            P(SP, "tp"),
            P(SP, "tp"),
            P(),
            P(),
            P("tp"),
            P("tp"),
            P(None, SP, "tp"),
            P(None, "tp"),
            P(None, "tp"),
            P(None, "tp"),
            P(None, "tp"),
            P(None, "tp"),
            P(),
            P("tp", SP),
        ),
        out_specs=(P(None, "tp", None, None), P(None, SP), P(None, SP, "tp", None, None)),
        check_vma=False,
    )
```

```python
import jax
import jax.numpy as jnp
from jax import lax
from jax.experimental import pallas as pl
from jax.experimental.pallas import tpu as pltpu
from jax.sharding import Mesh
from jax.sharding import PartitionSpec as P

WIDTH = 128
SIDE = 8
EPSILON = 1e-06
BEST = lax.Precision.HIGHEST
SP = ("z", "y")
INTERPRET = False
SMALL = pltpu.CompilerParams(vmem_limit_bytes=16 * 1024 * 1024)


def exchange(messages, axis):
    return lax.all_to_all(messages, axis, split_axis=0, concat_axis=0, tiled=True)


def from_everyone(array, axis):
    return exchange(jnp.broadcast_to(array, (lax.axis_size(axis), *array.shape)), axis)


def columns_body(tokens_ref, columns_ref):
    share = tokens_ref.shape[1] // (SIDE * SIDE)
    for to in range(SIDE):
        at = [(k * SIDE + to) * share for k in range(SIDE)]
        columns_ref[to] = jnp.concatenate([tokens_ref[:, a : a + share] for a in at], axis=1)


def columns_by_owner(flat):
    rows, model = flat.shape
    step = rows // 4
    return pl.pallas_call(
        columns_body,
        grid=(rows // step,),
        in_specs=[pl.BlockSpec((step, model), lambda i: (i, 0))],
        out_specs=pl.BlockSpec((SIDE, step, model // SIDE), lambda i: (0, i, 0)),
        out_shape=jax.ShapeDtypeStruct((SIDE, rows, model // SIDE), flat.dtype),
        interpret=INTERPRET,
        compiler_params=SMALL,
        name="columns",
    )(flat)


VMEM = pl.BlockSpec(memory_space=pltpu.VMEM)


def partial_body(tokens_ref, weights_ref, gates_ref, sent_ref):
    line, rows, _ = tokens_ref.shape
    owners, halves, sent_rows, width = sent_ref.shape
    ranges = line // halves
    positions = (sent_rows - gates_ref.shape[2]) // ranges
    prompts = rows // positions
    heads = owners // prompts
    for k in range(line):
        half, j = k // ranges, k % ranges
        part = jnp.dot(tokens_ref[k], weights_ref[...], preferred_element_type=jnp.float32)
        part = part.astype(sent_ref.dtype)
        for p in range(prompts):
            for h in range(heads):
                sent_ref[p * heads + h, half, j * positions : (j + 1) * positions, :] = part[
                    p * positions : (p + 1) * positions, h * width : (h + 1) * width
                ]
    sent_ref[:, :, ranges * positions :, :] = gates_ref[...]


def partial_projections(tokens, weights, gates, positions):
    owners, halves, extra, width = gates.shape
    sent_rows = tokens.shape[0] // halves * positions + extra
    return pl.pallas_call(
        partial_body,
        in_specs=[VMEM, VMEM, VMEM],
        out_specs=VMEM,
        out_shape=jax.ShapeDtypeStruct((owners, halves, sent_rows, width), tokens.dtype),
        interpret=INTERPRET,
        compiler_params=SMALL,
        name="partials",
    )(tokens, weights, gates)


def unit_inverse(lower_part):
    order = lower_part.shape[-1]
    identity = jnp.eye(order, dtype=jnp.float32)
    result = identity - lower_part
    power = lower_part
    reached = 2
    while reached < order:
        power = jnp.matmul(power, power, precision=BEST)
        result = jnp.matmul(result, identity + power, precision=BEST)
        reached *= 2
    return result


def two_parts(values):
    high = lax.reduce_precision(values, 8, 7)
    return high.astype(jnp.bfloat16), (values - high).astype(jnp.bfloat16)


def range_maps(keys, values, beta, fading):
    block = keys.shape[1]
    cumulative = jnp.cumsum(fading, axis=-1)
    at = jnp.arange(block)
    strict = at[:, None] > at[None, :]
    spread = jnp.where(strict, cumulative[:, :, None] - cumulative[:, None, :], 0.0)
    scaled = keys * beta[..., None]
    inner = jnp.einsum("nik,njk->nij", scaled, keys, precision=BEST)
    inverse = unit_inverse(jnp.where(strict, inner * jnp.exp(spread), 0.0))
    targets = jnp.concatenate(
        [scaled * jnp.exp(cumulative)[..., None], values * beta[..., None]], axis=-1
    )
    solved = jnp.einsum("nij,njk->nik", inverse, targets, precision=BEST)
    last = cumulative[:, -1:]
    tail = keys * jnp.exp(last - cumulative)[..., None]
    moved = jnp.einsum("njk,njw->nkw", tail, solved, precision=BEST)
    identity = jnp.eye(WIDTH, dtype=jnp.float32)
    transition = jnp.exp(last)[..., None] * identity - moved[..., :WIDTH]
    return jnp.concatenate([transition, moved[..., WIDTH:]], axis=-1)


def then(earlier, later):
    both = jnp.matmul(later[..., :WIDTH], earlier, precision=BEST)
    return jnp.concatenate([both[..., :WIDTH], both[..., WIDTH:] + later[..., WIDTH:]], axis=-1)


def applied(maps, state):
    return jnp.matmul(maps[..., :WIDTH], state, precision=BEST) + maps[..., WIDTH:]


def read_heads(state_cache, probe, address, content, outgate, strength_raw, gain):
    prompts, heads, width, _ = state_cache.shape
    state = state_cache.astype(jnp.float32)

    def activate(tensor):
        return jax.nn.silu(tensor.astype(jnp.float32)).reshape(prompts, heads, width)

    query = activate(probe)
    key = activate(address)
    key = key * lax.rsqrt(jnp.sum(key * key, axis=-1, keepdims=True) + EPSILON)
    value = activate(content)
    strength = jax.nn.sigmoid(strength_raw)
    recalled = jnp.einsum("nhk,nhkv->nhv", key, state, precision=BEST)
    updated = state + strength[..., None, None] * key[..., :, None] * (value - recalled)[..., None, :]
    output = jnp.einsum("nhk,nhkv->nhv", query, updated, precision=BEST)
    normed = output * lax.rsqrt(jnp.mean(output * output, axis=-1, keepdims=True) + EPSILON) * gain
    return (normed * activate(outgate)).reshape(prompts, heads * width).astype(jnp.bfloat16)


def per_device(
    tokens,
    address_projection,
    content_projection,
    strength_projection,
    fading_driver_projection,
    strength_offset,
    fading_speed,
    added_fading,
    probe,
    address,
    content,
    outgate,
    strength_raw,
    gain,
    readout_projection,
):
    prompts, positions, model = tokens.shape
    heads = fading_speed.shape[0]
    rows = prompts * positions
    share = model // (SIDE * SIDE)
    z, y, tp = lax.axis_index("z"), lax.axis_index("y"), lax.axis_index("tp")
    half = SIDE // 2
    my_half = y % 2

    weights = jnp.concatenate(
        [
            part[:, head * WIDTH : (head + 1) * WIDTH]
            for head in range(heads)
            for part in (address_projection, content_projection)
        ],
        axis=1,
    )
    flat = tokens.reshape(rows, model)
    columns = columns_by_owner(flat)
    line_tokens = exchange(columns, "y")
    line_weights = lax.all_gather(weights, "z", axis=0, tiled=True)

    drivers = jnp.concatenate([strength_projection, fading_driver_projection], axis=1)
    logits = jnp.dot(flat, drivers, preferred_element_type=jnp.float32).astype(jnp.bfloat16)
    logits = logits.astype(jnp.float32).reshape(prompts, positions, 2, -1)
    mine = lax.dynamic_slice_in_dim(logits, tp * heads, heads, 3)
    beta = jax.nn.sigmoid(mine[:, :, 0] + strength_offset)
    fading = added_fading - fading_speed * jax.nn.softplus(mine[:, :, 1])
    gates = jnp.stack([*two_parts(beta), *two_parts(fading)])
    gates = gates.transpose(1, 3, 0, 2).reshape(prompts, heads, 1, 1, 4 * positions)

    gates = jnp.broadcast_to(gates, (prompts, heads, 2, 16, 4 * positions))
    sent = partial_projections(
        line_tokens,
        line_weights,
        gates.reshape(prompts * heads, 2, 16, 4 * positions),
        positions,
    ).reshape(SIDE, half * positions + 16, 4 * positions)
    got = exchange(sent, "y")

    sums = got[:, : half * positions].astype(jnp.float32).sum(axis=0)
    sums = sums.reshape(half, positions, 2 * WIDTH)
    gates = lax.dynamic_slice_in_dim(got[:, half * positions], my_half * half, half, 0)
    gates = gates.astype(jnp.float32).reshape(half, 4, positions)
    beta = gates[:, 0] + gates[:, 1]
    fading = gates[:, 2] + gates[:, 3]
    keys = jax.nn.silu(sums[..., :WIDTH])
    keys = keys * lax.rsqrt(jnp.sum(keys * keys, axis=-1, keepdims=True) + EPSILON)
    values = jax.nn.silu(sums[..., WIDTH:])
    maps = range_maps(keys, values, beta, fading)
    inside = [maps[0]]
    for j in range(1, half):
        inside.append(then(inside[-1], maps[j]))

    whole = inside[-1].astype(jnp.bfloat16)
    other = lax.ppermute(whole, "y", [(i, i ^ 1) for i in range(SIDE)])
    first = jnp.where(my_half == 0, whole, other).astype(jnp.float32)
    second = jnp.where(my_half == 0, other, whole).astype(jnp.float32)
    line = then(first, second).astype(jnp.bfloat16)
    lines = from_everyone(line, "z").astype(jnp.float32)
    state = jnp.zeros((WIDTH, WIDTH), jnp.float32)
    entering = state
    for k in range(SIDE):
        entering = jnp.where(z == k, state, entering)
        state = applied(lines[k], state) if k else lines[0][:, WIDTH:]
    entering = jnp.where(my_half == 0, entering, applied(first, entering))
    leaving = applied(jnp.stack(inside), entering).astype(jnp.bfloat16)

    final_half = lax.dynamic_slice_in_dim(
        state.astype(jnp.bfloat16), my_half * (WIDTH // 2), WIDTH // 2, 0
    )
    home = jnp.concatenate(
        [
            jnp.concatenate([leaving, leaving], axis=0),
            jnp.broadcast_to(final_half, (SIDE, *final_half.shape)),
        ],
        axis=1,
    )
    back = exchange(home, "y").reshape(prompts, heads, 2, WIDTH + WIDTH // 2, WIDTH)
    boundary = lax.dynamic_index_in_dim(back, y // half, 2, keepdims=False)[:, :, :WIDTH]
    state_cache = back[:, :, :, WIDTH:].reshape(prompts, heads, WIDTH, WIDTH)

    heads_read = read_heads(state_cache, probe, address, content, outgate, strength_raw, gain)
    terms = jnp.dot(heads_read, readout_projection, preferred_element_type=jnp.float32)
    mixed = from_everyone(terms.astype(jnp.bfloat16), "tp").astype(jnp.float32).sum(axis=0)
    return state_cache, mixed.astype(jnp.bfloat16), boundary[:, None]


def solution(mesh):
    finer = Mesh(mesh.devices.reshape(SIDE, SIDE, mesh.shape["tp"]), (*SP, "tp"))
    return jax.shard_map(
        per_device,
        mesh=finer,
        in_specs=(
            P(None, SP, None),
            P(SP, "tp"),
            P(SP, "tp"),
            P(),
            P(),
            P("tp"),
            P("tp"),
            P(None, SP, "tp"),
            P(None, "tp"),
            P(None, "tp"),
            P(None, "tp"),
            P(None, "tp"),
            P(None, "tp"),
            P(),
            P("tp", SP),
        ),
        out_specs=(P(None, "tp", None, None), P(None, SP), P(None, SP, "tp", None, None)),
        check_vma=False,
    )
```

```python
import jax
import jax.numpy as jnp
from jax import lax
from jax.experimental import pallas as pl
from jax.experimental.pallas import tpu as pltpu
from jax.sharding import Mesh
from jax.sharding import PartitionSpec as P

WIDTH = 128
SIDE = 8
EPSILON = 1e-06
BEST = lax.Precision.HIGHEST
SP = ("z", "y")
INTERPRET = False
SMALL = pltpu.CompilerParams(vmem_limit_bytes=16 * 1024 * 1024)


def exchange(messages, axis):
    return lax.all_to_all(messages, axis, split_axis=0, concat_axis=0, tiled=True)


def columns_body(tokens_ref, columns_ref):
    share = tokens_ref.shape[1] // (SIDE * SIDE)
    for to in range(SIDE):
        at = [(k * SIDE + to) * share for k in range(SIDE)]
        columns_ref[to] = jnp.concatenate([tokens_ref[:, a : a + share] for a in at], axis=1)


def columns_by_owner(flat):
    rows, model = flat.shape
    step = rows // 4
    return pl.pallas_call(
        columns_body,
        grid=(rows // step,),
        in_specs=[pl.BlockSpec((step, model), lambda i: (i, 0))],
        out_specs=pl.BlockSpec((SIDE, step, model // SIDE), lambda i: (0, i, 0)),
        out_shape=jax.ShapeDtypeStruct((SIDE, rows, model // SIDE), flat.dtype),
        interpret=INTERPRET,
        compiler_params=SMALL,
        name="columns",
    )(flat)


VMEM = pl.BlockSpec(memory_space=pltpu.VMEM)


def partial_body(tokens_ref, weights_ref, gates_ref, sent_ref):
    line, rows, _ = tokens_ref.shape
    owners, halves, sent_rows, width = sent_ref.shape
    ranges = line // halves
    positions = (sent_rows - gates_ref.shape[2]) // ranges
    prompts = rows // positions
    heads = owners // prompts
    for k in range(line):
        half, j = k // ranges, k % ranges
        part = jnp.dot(tokens_ref[k], weights_ref[...], preferred_element_type=jnp.float32)
        part = part.astype(sent_ref.dtype)
        for p in range(prompts):
            for h in range(heads):
                sent_ref[p * heads + h, half, j * positions : (j + 1) * positions, :] = part[
                    p * positions : (p + 1) * positions, h * width : (h + 1) * width
                ]
    sent_ref[:, :, ranges * positions :, :] = gates_ref[...]


def partial_projections(tokens, weights, gates, positions):
    owners, halves, extra, width = gates.shape
    sent_rows = tokens.shape[0] // halves * positions + extra
    return pl.pallas_call(
        partial_body,
        in_specs=[VMEM, VMEM, VMEM],
        out_specs=VMEM,
        out_shape=jax.ShapeDtypeStruct((owners, halves, sent_rows, width), tokens.dtype),
        interpret=INTERPRET,
        compiler_params=SMALL,
        name="partials",
    )(tokens, weights, gates)


def two_parts(values):
    high = lax.reduce_precision(values, 8, 7)
    return high.astype(jnp.bfloat16), (values - high).astype(jnp.bfloat16)


def best(left, right, dims=((1,), (0,))):
    return lax.dot_general(
        left, right, (dims, ((), ())), precision=BEST, preferred_element_type=jnp.float32
    )


def times(state, matrix):
    high = state.astype(jnp.bfloat16)
    low = (state - high.astype(jnp.float32)).astype(jnp.bfloat16)
    rows = state.shape[0]
    both = jnp.dot(
        jnp.concatenate([high, low], axis=0), matrix, preferred_element_type=jnp.float32
    )
    return both[:rows] + both[rows:]


def silu(x):
    return x / (1.0 + jnp.exp(-x))


def ranges_body(half_ref, got_ref, sent_ref, kept_ref):
    line, _, width = got_ref.shape
    wide = width // 2
    ranges = line // 2
    positions = sent_ref.shape[0] // (ranges * 3)
    count = ranges * positions
    half = half_ref[0]
    sums = got_ref[0, :count, :].astype(jnp.float32)
    for k in range(1, line):
        sums = sums + got_ref[k, :count, :].astype(jnp.float32)
    keys = silu(sums[:, :wide])
    keys = keys * lax.rsqrt(jnp.sum(keys * keys, axis=-1, keepdims=True) + EPSILON)
    values = silu(sums[:, wide:])
    gates = got_ref[pl.ds(half * ranges, ranges), count:, :wide].astype(jnp.float32)
    beta = gates[:, 0, :] + gates[:, 1, :]
    fading = gates[:, 2, :] + gates[:, 3, :]
    up_to = lax.broadcasted_iota(jnp.int32, (wide, wide), 0) <= lax.broadcasted_iota(
        jnp.int32, (wide, wide), 1
    )
    sums_to = best(jnp.concatenate([beta, fading], axis=0), up_to.astype(jnp.float32))[ranges:]
    columns = jnp.concatenate([beta, sums_to], axis=0).T
    row = lax.broadcasted_iota(jnp.int32, (positions, positions), 0)
    column = lax.broadcasted_iota(jnp.int32, (positions, positions), 1)
    strict = row > column
    unit = (
        lax.broadcasted_iota(jnp.int32, (wide, wide), 0)
        == lax.broadcasted_iota(jnp.int32, (wide, wide), 1)
    ).astype(jnp.float32)
    powers, solved, tails, lasts = [], [], [], []
    for j in range(ranges):
        at = slice(j * positions, (j + 1) * positions)
        b = columns[:positions, j : j + 1]
        total = columns[:positions, ranges + j : ranges + j + 1]
        last = total[positions - 1 :, :]
        across = sums_to[j : j + 1, :positions]
        scaled = keys[at] * b
        inner = best(scaled, keys[at], ((1,), (1,)))
        spread = jnp.exp(jnp.where(strict, total - across, 0.0))
        powers.append(jnp.where(strict, inner * spread, 0.0))
        solved.append(jnp.concatenate([scaled * jnp.exp(total), values[at] * b], axis=1))
        tails.append(keys[at] * jnp.exp(last - total))
        lasts.append(jnp.exp(last))
    for j in range(ranges):
        solved[j] = solved[j] - best(powers[j], solved[j])
    reached = 2
    while reached < positions:
        for j in range(ranges):
            powers[j] = best(powers[j], powers[j])
        for j in range(ranges):
            solved[j] = solved[j] + best(powers[j], solved[j])
        reached *= 2
    so_far = None
    for j in range(ranges):
        moved = best(solved[j], tails[j], ((0,), (0,)))
        step = lasts[j] * unit - moved[:wide]
        if so_far is None:
            so_far = jnp.concatenate([step, moved[wide:]], axis=0)
        else:
            both = best(so_far, step)
            so_far = jnp.concatenate([both[:wide], both[wide:] + moved[wide:]], axis=0)
        out = so_far.astype(jnp.bfloat16)
        low, high = out[wide : wide + positions], out[wide + positions :]
        sent_ref[j * wide : (j + 1) * wide, :] = out[:wide]
        at = slice(ranges * wide + j * positions, ranges * wide + (j + 1) * positions)
        sent_ref[at, :] = jnp.where(half == 0, high, low)
        kept_ref[j * wide : (j + 1) * wide, :] = out[:wide]
        kept_ref[at, :] = jnp.where(half == 0, low, high)


def line_body(half_ref, kept_ref, other_ref, sent_ref):
    count, wide = kept_ref.shape
    ranges = 2 * count // (3 * wide)
    rows = wide // 2
    mine_first = half_ref[0] == 0
    step = slice((ranges - 1) * wide, ranges * wide)
    kept = jnp.concatenate([kept_ref[step, :], kept_ref[count - rows :, :]], axis=0)
    other = jnp.concatenate([other_ref[step, :], other_ref[count - rows :, :]], axis=0)
    first = jnp.where(mine_first, kept, other)
    second = jnp.where(mine_first, other, kept)
    both = jnp.dot(first, second[:wide], preferred_element_type=jnp.float32)
    added = both[wide:] + second[wide:].astype(jnp.float32)
    out = jnp.concatenate([both[:wide], added], axis=0).astype(jnp.bfloat16)
    for k in range(sent_ref.shape[0]):
        sent_ref[k] = out


def scan_body(place_ref, lines_ref, kept_ref, other_ref, sent_ref):
    lines, _, wide = lines_ref.shape
    rows = wide // 2
    ranges = sent_ref.shape[0] // 2
    z, mine_first = place_ref[0], place_ref[1] == 0
    state = lines_ref[0, wide:, :].astype(jnp.float32)
    entering = jnp.zeros_like(state)
    for k in range(1, lines):
        entering = jnp.where(z == k, state, entering)
        state = times(state, lines_ref[k, :wide, :]) + lines_ref[k, wide:, :].astype(jnp.float32)
    final = state.astype(jnp.bfloat16)
    state = entering
    for h in range(2):
        begin = state
        for j in range(ranges):
            step = slice(j * wide, (j + 1) * wide)
            extra = slice(ranges * wide + j * rows, ranges * wide + (j + 1) * rows)
            use_kept = mine_first if h == 0 else jnp.logical_not(mine_first)
            matrix = jnp.where(use_kept, kept_ref[step, :], other_ref[step, :])
            added = jnp.where(use_kept, kept_ref[extra, :], other_ref[extra, :])
            state = times(begin, matrix) + added.astype(jnp.float32)
            sent_ref[h * ranges + j, :rows, :] = state.astype(jnp.bfloat16)
            sent_ref[h * ranges + j, rows:, :] = final


def read_body(
    strength_ref,
    back_ref,
    probe_ref,
    address_ref,
    content_ref,
    outgate_ref,
    gain_ref,
    readout_ref,
    sent_ref,
):
    wide = back_ref.shape[2]
    rows = wide // 2
    prompts, width = probe_ref.shape
    heads = width // wide
    read = []
    for p in range(prompts):
        for h in range(heads):
            at, n = slice(h * wide, (h + 1) * wide), 2 * (p * heads + h)
            state = jnp.concatenate([back_ref[n, rows:, :], back_ref[n + 1, rows:, :]], axis=0)
            query = silu(probe_ref[p : p + 1, at].astype(jnp.float32))
            key = silu(address_ref[p : p + 1, at].astype(jnp.float32))
            key = key * lax.rsqrt(jnp.sum(key * key, axis=-1, keepdims=True) + EPSILON)
            value = silu(content_ref[p : p + 1, at].astype(jnp.float32))
            strength = 1.0 / (1.0 + jnp.exp(-jnp.full((1, 1), strength_ref[p, h], jnp.float32)))
            pair = jnp.concatenate([key, query, jnp.zeros((6, wide), jnp.float32)], axis=0)
            found = best(pair, state.astype(jnp.float32), ((1,), (1,)))
            along = jnp.sum(key * query, axis=-1, keepdims=True)
            out = found[1:2] + strength * along * (value - found[0:1])
            out = out * lax.rsqrt(jnp.mean(out * out, axis=-1, keepdims=True) + EPSILON)
            read.append(out * gain_ref[...] * silu(outgate_ref[p : p + 1, at].astype(jnp.float32)))
    rows_of = [jnp.concatenate(read[p * heads : (p + 1) * heads], axis=1) for p in range(prompts)]
    heads_read = jnp.concatenate(rows_of, axis=0).astype(jnp.bfloat16)
    terms = jnp.dot(heads_read, readout_ref[...], preferred_element_type=jnp.float32)
    for k in range(sent_ref.shape[0]):
        sent_ref[k] = terms.astype(jnp.bfloat16)


SMEM = pl.BlockSpec(memory_space=pltpu.SMEM)


def local(body, name, shapes, *operands):
    out = [jax.ShapeDtypeStruct(shape, jnp.bfloat16) for shape in shapes]
    return pl.pallas_call(
        body,
        in_specs=[SMEM] + [VMEM] * (len(operands) - 1),
        out_specs=[VMEM] * len(out),
        out_shape=out,
        interpret=INTERPRET,
        compiler_params=SMALL,
        name=name,
    )(*operands)


def per_device(
    tokens,
    address_projection,
    content_projection,
    strength_projection,
    fading_driver_projection,
    strength_offset,
    fading_speed,
    added_fading,
    probe,
    address,
    content,
    outgate,
    strength_raw,
    gain,
    readout_projection,
):
    prompts, positions, model = tokens.shape
    heads = fading_speed.shape[0]
    rows = prompts * positions
    share = model // (SIDE * SIDE)
    z, y, tp = lax.axis_index("z"), lax.axis_index("y"), lax.axis_index("tp")
    half = SIDE // 2
    my_half = y % 2

    weights = jnp.concatenate(
        [
            part[:, head * WIDTH : (head + 1) * WIDTH]
            for head in range(heads)
            for part in (address_projection, content_projection)
        ],
        axis=1,
    )
    flat = tokens.reshape(rows, model)
    columns = columns_by_owner(flat)
    line_tokens = exchange(columns, "y")
    line_weights = lax.all_gather(weights, "z", axis=0, tiled=True)

    drivers = jnp.concatenate([strength_projection, fading_driver_projection], axis=1)
    logits = jnp.dot(flat, drivers, preferred_element_type=jnp.float32).astype(jnp.bfloat16)
    logits = logits.astype(jnp.float32).reshape(prompts, positions, 2, -1)
    mine = lax.dynamic_slice_in_dim(logits, tp * heads, heads, 3)
    beta = jax.nn.sigmoid(mine[:, :, 0] + strength_offset)
    fading = added_fading - fading_speed * jax.nn.softplus(mine[:, :, 1])
    gates = jnp.stack([*two_parts(beta), *two_parts(fading)])
    gates = jnp.pad(
        gates.transpose(1, 3, 0, 2), ((0, 0), (0, 0), (0, 12), (0, 2 * WIDTH - positions))
    )

    gates = jnp.broadcast_to(gates[:, :, None], (prompts, heads, 2, *gates.shape[2:]))
    sent = partial_projections(
        line_tokens,
        line_weights,
        gates.reshape(prompts * heads, *gates.shape[2:]),
        positions,
    )
    got = exchange(sent.reshape(SIDE, *sent.shape[2:]), "y")

    side = my_half.astype(jnp.int32).reshape(1)
    size = (half * (WIDTH + WIDTH // 2), WIDTH)
    given, kept = local(ranges_body, "ranges", [size, size], side, got)
    other = lax.ppermute(given, "y", [(i, i ^ 1) for i in range(SIDE)])
    (line,) = local(line_body, "line", [(SIDE, WIDTH + WIDTH // 2, WIDTH)], side, kept, other)
    lines = exchange(line, "z")
    place = jnp.stack([z, my_half]).astype(jnp.int32)
    (home,) = local(scan_body, "scan", [(SIDE, WIDTH, WIDTH)], place, lines, kept, other)

    back = exchange(home, "y")
    (terms,) = local(
        read_body,
        "read",
        [(lax.axis_size("tp"), prompts, readout_projection.shape[1])],
        strength_raw,
        back,
        probe,
        address,
        content,
        outgate,
        gain.reshape(1, WIDTH),
        readout_projection,
    )
    mixed = exchange(terms, "tp").astype(jnp.float32).sum(axis=0)
    states = back.reshape(prompts, heads, 2, 2, WIDTH // 2, WIDTH).transpose(3, 0, 1, 5, 2, 4)
    boundary, state_cache = states.reshape(2, prompts, heads, WIDTH, WIDTH)
    return state_cache, mixed.astype(jnp.bfloat16), boundary[:, None]


def solution(mesh):
    finer = Mesh(mesh.devices.reshape(SIDE, SIDE, mesh.shape["tp"]), (*SP, "tp"))
    return jax.shard_map(
        per_device,
        mesh=finer,
        in_specs=(
            P(None, SP, None),
            P(SP, "tp"),
            P(SP, "tp"),
            P(),
            P(),
            P("tp"),
            P("tp"),
            P(None, SP, "tp"),
            P(None, "tp"),
            P(None, "tp"),
            P(None, "tp"),
            P(None, "tp"),
            P(None, "tp"),
            P(),
            P("tp", SP),
        ),
        out_specs=(P(None, "tp", None, None), P(None, SP), P(None, SP, "tp", None, None)),
        check_vma=False,
    )
```

```python
import jax
import jax.numpy as jnp
from jax import lax
from jax.experimental import pallas as pl
from jax.experimental.pallas import tpu as pltpu
from jax.sharding import Mesh
from jax.sharding import PartitionSpec as P

WIDTH = 128
SIDE = 8
EPSILON = 1e-06
BEST = lax.Precision.HIGHEST
SP = ("z", "y")
INTERPRET = False
VMEM = pl.BlockSpec(memory_space=pltpu.VMEM)
SMALL = pltpu.CompilerParams(vmem_limit_bytes=16 * 1024 * 1024)


def exchange(messages, axis):
    return lax.all_to_all(messages, axis, split_axis=0, concat_axis=0, tiled=True)


def columns_body(tokens_ref, columns_ref, buffer_ref, arrived):
    parts, step, model = buffer_ref.shape
    share = model // (SIDE * SIDE)
    reads = [
        pltpu.make_async_copy(
            tokens_ref.at[i * step : (i + 1) * step, :], buffer_ref.at[i], arrived.at[i]
        )
        for i in range(parts)
    ]
    for read in reads:
        read.start()
    for i in range(parts):
        reads[i].wait()
        rows = buffer_ref[i]
        for to in range(SIDE):
            at = [(k * SIDE + to) * share for k in range(SIDE)]
            columns_ref[to, i * step : (i + 1) * step, :] = jnp.concatenate(
                [rows[:, a : a + share] for a in at], axis=1
            )


def columns_by_owner(flat, parts=4):
    rows, model = flat.shape
    return pl.pallas_call(
        columns_body,
        in_specs=[pl.BlockSpec(memory_space=pltpu.MemorySpace.HBM)],
        out_specs=VMEM,
        out_shape=jax.ShapeDtypeStruct((SIDE, rows, model // SIDE), flat.dtype),
        scratch_shapes=[
            pltpu.VMEM((parts, rows // parts, model), flat.dtype),
            pltpu.SemaphoreType.DMA((parts,)),
        ],
        interpret=INTERPRET,
        name="columns",
    )(flat)


def partial_body(tokens_ref, weights_ref, gates_ref, sent_ref):
    line, rows, _ = tokens_ref.shape
    owners, halves, sent_rows, width = sent_ref.shape
    ranges = line // halves
    positions = (sent_rows - gates_ref.shape[2]) // ranges
    prompts = rows // positions
    heads = owners // prompts
    for k in range(line):
        half, j = k // ranges, k % ranges
        part = jnp.dot(tokens_ref[k], weights_ref[...], preferred_element_type=jnp.float32)
        part = part.astype(sent_ref.dtype)
        for p in range(prompts):
            for h in range(heads):
                sent_ref[p * heads + h, half, j * positions : (j + 1) * positions, :] = part[
                    p * positions : (p + 1) * positions, h * width : (h + 1) * width
                ]
    sent_ref[:, :, ranges * positions :, :] = gates_ref[...]


def partial_projections(tokens, weights, gates, positions):
    owners, halves, extra, width = gates.shape
    sent_rows = tokens.shape[0] // halves * positions + extra
    return pl.pallas_call(
        partial_body,
        in_specs=[VMEM, VMEM, VMEM],
        out_specs=VMEM,
        out_shape=jax.ShapeDtypeStruct((owners, halves, sent_rows, width), tokens.dtype),
        interpret=INTERPRET,
        compiler_params=SMALL,
        name="partials",
    )(tokens, weights, gates)


def two_parts(values):
    high = lax.reduce_precision(values, 8, 7)
    return high.astype(jnp.bfloat16), (values - high).astype(jnp.bfloat16)


def best(left, right, dims=((1,), (0,))):
    return lax.dot_general(
        left, right, (dims, ((), ())), precision=BEST, preferred_element_type=jnp.float32
    )


def parts(x):
    high = x.astype(jnp.bfloat16)
    return high, (x - high.astype(jnp.float32)).astype(jnp.bfloat16)


def times(state, matrix):
    rows = state.shape[0]
    both = jnp.dot(
        jnp.concatenate(parts(state), axis=0), matrix, preferred_element_type=jnp.float32
    )
    return both[:rows] + both[rows:]


def near(left, right, dims=((1,), (0,))):
    (a, b), (c, d) = parts(left), parts(right)

    def dot(u, v):
        return lax.dot_general(u, v, (dims, ((), ())), preferred_element_type=jnp.float32)

    return dot(a, c) + (dot(a, d) + dot(b, c))


def silu(x):
    return x / (1.0 + jnp.exp(-x))


def ranges_body(half_ref, got_ref, sent_ref, kept_ref):
    line, _, width = got_ref.shape
    wide = width // 2
    ranges = line // 2
    positions = sent_ref.shape[0] // (ranges * 3)
    count = ranges * positions
    half = half_ref[0]
    sums = got_ref[0, :count, :].astype(jnp.float32)
    for k in range(1, line):
        sums = sums + got_ref[k, :count, :].astype(jnp.float32)
    keys = silu(sums[:, :wide])
    keys = keys * lax.rsqrt(jnp.sum(keys * keys, axis=-1, keepdims=True) + EPSILON)
    values = silu(sums[:, wide:])
    gates = got_ref[pl.ds(half * ranges, ranges), count:, :wide].astype(jnp.float32)
    beta = gates[:, 0, :] + gates[:, 1, :]
    fading = gates[:, 2, :] + gates[:, 3, :]
    up_to = lax.broadcasted_iota(jnp.int32, (wide, wide), 0) <= lax.broadcasted_iota(
        jnp.int32, (wide, wide), 1
    )
    sums_to = best(jnp.concatenate([beta, fading], axis=0), up_to.astype(jnp.float32))[ranges:]
    columns = jnp.concatenate([beta, sums_to], axis=0).T
    row = lax.broadcasted_iota(jnp.int32, (positions, positions), 0)
    column = lax.broadcasted_iota(jnp.int32, (positions, positions), 1)
    strict = row > column
    unit = (
        lax.broadcasted_iota(jnp.int32, (wide, wide), 0)
        == lax.broadcasted_iota(jnp.int32, (wide, wide), 1)
    ).astype(jnp.float32)
    powers, solved, tails, lasts = [], [], [], []
    for j in range(ranges):
        at = slice(j * positions, (j + 1) * positions)
        b = columns[:positions, j : j + 1]
        total = columns[:positions, ranges + j : ranges + j + 1]
        last = total[positions - 1 :, :]
        across = sums_to[j : j + 1, :positions]
        scaled = keys[at] * b
        inner = best(scaled, keys[at], ((1,), (1,)))
        spread = jnp.exp(jnp.where(strict, total - across, 0.0))
        powers.append(jnp.where(strict, inner * spread, 0.0))
        solved.append(jnp.concatenate([scaled * jnp.exp(total), values[at] * b], axis=1))
        tails.append(keys[at] * jnp.exp(last - total))
        lasts.append(jnp.exp(last))
    for j in range(ranges):
        solved[j] = solved[j] - best(powers[j], solved[j])
    reached = 2
    while reached < positions:
        for j in range(ranges):
            powers[j] = best(powers[j], powers[j])
        for j in range(ranges):
            solved[j] = solved[j] + best(powers[j], solved[j])
        reached *= 2
    so_far = None
    for j in range(ranges):
        moved = near(solved[j], tails[j], ((0,), (0,)))
        step = lasts[j] * unit - moved[:wide]
        if so_far is None:
            so_far = jnp.concatenate([step, moved[wide:]], axis=0)
        else:
            both = near(so_far, step)
            so_far = jnp.concatenate([both[:wide], both[wide:] + moved[wide:]], axis=0)
        out = so_far.astype(jnp.bfloat16)
        low, high = out[wide : wide + positions], out[wide + positions :]
        sent_ref[j * wide : (j + 1) * wide, :] = out[:wide]
        at = slice(ranges * wide + j * positions, ranges * wide + (j + 1) * positions)
        sent_ref[at, :] = jnp.where(half == 0, high, low)
        kept_ref[j * wide : (j + 1) * wide, :] = out[:wide]
        kept_ref[at, :] = jnp.where(half == 0, low, high)


def line_body(half_ref, kept_ref, other_ref, sent_ref):
    count, wide = kept_ref.shape
    ranges = 2 * count // (3 * wide)
    rows = wide // 2
    mine_first = half_ref[0] == 0
    step = slice((ranges - 1) * wide, ranges * wide)
    kept = jnp.concatenate([kept_ref[step, :], kept_ref[count - rows :, :]], axis=0)
    other = jnp.concatenate([other_ref[step, :], other_ref[count - rows :, :]], axis=0)
    first = jnp.where(mine_first, kept, other)
    second = jnp.where(mine_first, other, kept)
    both = jnp.dot(first, second[:wide], preferred_element_type=jnp.float32)
    added = both[wide:] + second[wide:].astype(jnp.float32)
    out = jnp.concatenate([both[:wide], added], axis=0).astype(jnp.bfloat16)
    for k in range(sent_ref.shape[0]):
        sent_ref[k] = out


def scan_body(place_ref, lines_ref, kept_ref, other_ref, sent_ref):
    lines, _, wide = lines_ref.shape
    rows = wide // 2
    ranges = sent_ref.shape[0] // 2
    z, mine_first = place_ref[0], place_ref[1] == 0
    state = lines_ref[0, wide:, :].astype(jnp.float32)
    entering = jnp.zeros_like(state)
    for k in range(1, lines):
        entering = jnp.where(z == k, state, entering)
        state = times(state, lines_ref[k, :wide, :]) + lines_ref[k, wide:, :].astype(jnp.float32)
    final = state.astype(jnp.bfloat16)
    state = entering
    for h in range(2):
        begin = state
        for j in range(ranges):
            step = slice(j * wide, (j + 1) * wide)
            extra = slice(ranges * wide + j * rows, ranges * wide + (j + 1) * rows)
            use_kept = mine_first if h == 0 else jnp.logical_not(mine_first)
            matrix = jnp.where(use_kept, kept_ref[step, :], other_ref[step, :])
            added = jnp.where(use_kept, kept_ref[extra, :], other_ref[extra, :])
            state = times(begin, matrix) + added.astype(jnp.float32)
            sent_ref[h * ranges + j, :rows, :] = state.astype(jnp.bfloat16)
            sent_ref[h * ranges + j, rows:, :] = final


def read_body(
    strength_ref,
    back_ref,
    probe_ref,
    address_ref,
    content_ref,
    outgate_ref,
    gain_ref,
    readout_ref,
    sent_ref,
):
    wide = back_ref.shape[2]
    rows = wide // 2
    prompts, width = probe_ref.shape
    heads = width // wide
    each = [(p, h) for p in range(prompts) for h in range(heads)]

    def gathered(ref):
        wanted = [ref[p : p + 1, h * wide : (h + 1) * wide] for p, h in each]
        return jnp.concatenate(wanted, axis=0).astype(jnp.float32)

    query = silu(gathered(probe_ref))
    key = silu(gathered(address_ref))
    key = key * lax.rsqrt(jnp.sum(key * key, axis=-1, keepdims=True) + EPSILON)
    value = silu(gathered(content_ref))
    strength = jnp.concatenate(
        [jnp.full((1, 1), strength_ref[p, h], jnp.float32) for p, h in each], axis=0
    )
    strength = 1.0 / (1.0 + jnp.exp(-strength))
    pair = jnp.concatenate([key, query], axis=0)
    recalled, probed = [], []
    for n in range(len(each)):
        state = jnp.concatenate([back_ref[2 * n, rows:, :], back_ref[2 * n + 1, rows:, :]], axis=0)
        found = best(pair, state.astype(jnp.float32), ((1,), (1,)))
        recalled.append(found[n : n + 1])
        probed.append(found[len(each) + n : len(each) + n + 1])
    along = jnp.sum(key * query, axis=-1, keepdims=True)
    out = jnp.concatenate(probed, axis=0) + strength * along * (
        value - jnp.concatenate(recalled, axis=0)
    )
    out = out * lax.rsqrt(jnp.mean(out * out, axis=-1, keepdims=True) + EPSILON)
    read = out * gain_ref[...] * silu(gathered(outgate_ref))
    rows_of = [
        jnp.concatenate([read[p * heads + h :][:1] for h in range(heads)], axis=1)
        for p in range(prompts)
    ]
    heads_read = jnp.concatenate(rows_of, axis=0).astype(jnp.bfloat16)
    terms = jnp.dot(heads_read, readout_ref[...], preferred_element_type=jnp.float32)
    for k in range(sent_ref.shape[0]):
        sent_ref[k] = terms.astype(jnp.bfloat16)


SMEM = pl.BlockSpec(memory_space=pltpu.SMEM)


def local(body, name, shapes, *operands):
    out = [jax.ShapeDtypeStruct(shape, jnp.bfloat16) for shape in shapes]
    return pl.pallas_call(
        body,
        in_specs=[SMEM] + [VMEM] * (len(operands) - 1),
        out_specs=[VMEM] * len(out),
        out_shape=out,
        interpret=INTERPRET,
        compiler_params=SMALL,
        name=name,
    )(*operands)


def per_device(
    tokens,
    address_projection,
    content_projection,
    strength_projection,
    fading_driver_projection,
    strength_offset,
    fading_speed,
    added_fading,
    probe,
    address,
    content,
    outgate,
    strength_raw,
    gain,
    readout_projection,
):
    prompts, positions, model = tokens.shape
    heads = fading_speed.shape[0]
    rows = prompts * positions
    share = model // (SIDE * SIDE)
    z, y, tp = lax.axis_index("z"), lax.axis_index("y"), lax.axis_index("tp")
    half = SIDE // 2
    my_half = y % 2

    weights = jnp.concatenate(
        [
            part[:, head * WIDTH : (head + 1) * WIDTH]
            for head in range(heads)
            for part in (address_projection, content_projection)
        ],
        axis=1,
    )
    flat = tokens.reshape(rows, model)
    columns = columns_by_owner(flat)
    line_tokens = exchange(columns, "y")
    line_weights = lax.all_gather(weights, "z", axis=0, tiled=True)

    drivers = jnp.concatenate([strength_projection, fading_driver_projection], axis=1)
    logits = jnp.dot(flat, drivers, preferred_element_type=jnp.float32).astype(jnp.bfloat16)
    logits = logits.astype(jnp.float32).reshape(prompts, positions, 2, -1)
    mine = lax.dynamic_slice_in_dim(logits, tp * heads, heads, 3)
    beta = jax.nn.sigmoid(mine[:, :, 0] + strength_offset)
    fading = added_fading - fading_speed * jax.nn.softplus(mine[:, :, 1])
    gates = jnp.stack([*two_parts(beta), *two_parts(fading)])
    gates = jnp.pad(
        gates.transpose(1, 3, 0, 2), ((0, 0), (0, 0), (0, 4), (0, 2 * WIDTH - positions))
    )

    gates = jnp.broadcast_to(gates[:, :, None], (prompts, heads, 2, *gates.shape[2:]))
    sent = partial_projections(
        line_tokens,
        line_weights,
        gates.reshape(prompts * heads, *gates.shape[2:]),
        positions,
    )
    got = exchange(sent.reshape(SIDE, *sent.shape[2:]), "y")

    side = my_half.astype(jnp.int32).reshape(1)
    size = (half * (WIDTH + WIDTH // 2), WIDTH)
    given, kept = local(ranges_body, "ranges", [size, size], side, got)
    other = lax.ppermute(given, "y", [(i, i ^ 1) for i in range(SIDE)])
    (line,) = local(line_body, "line", [(SIDE, WIDTH + WIDTH // 2, WIDTH)], side, kept, other)
    lines = exchange(line, "z")
    place = jnp.stack([z, my_half]).astype(jnp.int32)
    (home,) = local(scan_body, "scan", [(SIDE, WIDTH, WIDTH)], place, lines, kept, other)

    back = exchange(home, "y")
    (terms,) = local(
        read_body,
        "read",
        [(lax.axis_size("tp"), prompts, readout_projection.shape[1])],
        strength_raw,
        back,
        probe,
        address,
        content,
        outgate,
        gain.reshape(1, WIDTH),
        readout_projection,
    )
    mixed = exchange(terms, "tp").astype(jnp.float32).sum(axis=0)
    states = back.reshape(prompts, heads, 2, 2, WIDTH // 2, WIDTH).transpose(3, 0, 1, 5, 2, 4)
    boundary, state_cache = states.reshape(2, prompts, heads, WIDTH, WIDTH)
    return state_cache, mixed.astype(jnp.bfloat16), boundary[:, None]


def solution(mesh):
    finer = Mesh(mesh.devices.reshape(SIDE, SIDE, mesh.shape["tp"]), (*SP, "tp"))
    return jax.shard_map(
        per_device,
        mesh=finer,
        in_specs=(
            P(None, SP, None),
            P(SP, "tp"),
            P(SP, "tp"),
            P(),
            P(),
            P("tp"),
            P("tp"),
            P(None, SP, "tp"),
            P(None, "tp"),
            P(None, "tp"),
            P(None, "tp"),
            P(None, "tp"),
            P(None, "tp"),
            P(),
            P("tp", SP),
        ),
        out_specs=(P(None, "tp", None, None), P(None, SP), P(None, SP, "tp", None, None)),
        check_vma=False,
    )
```

```python
import jax
import jax.numpy as jnp
from jax import lax
from jax.experimental import pallas as pl
from jax.experimental.pallas import tpu as pltpu
from jax.sharding import Mesh
from jax.sharding import PartitionSpec as P

WIDTH = 128
SIDE = 8
EPSILON = 1e-06
BEST = lax.Precision.HIGHEST
Z = ("zh", "zl")
SP = (*Z, "y")
INTERPRET = False
VMEM = pl.BlockSpec(memory_space=pltpu.VMEM)
SMALL = pltpu.CompilerParams(vmem_limit_bytes=16 * 1024 * 1024)


def exchange(messages, axis):
    return lax.all_to_all(messages, axis, split_axis=0, concat_axis=0, tiled=True)


def columns_body(tokens_ref, columns_ref, buffer_ref, arrived):
    parts, step, model = buffer_ref.shape
    share = model // (SIDE * SIDE)
    reads = [
        pltpu.make_async_copy(
            tokens_ref.at[i * step : (i + 1) * step, :], buffer_ref.at[i], arrived.at[i]
        )
        for i in range(parts)
    ]
    for read in reads:
        read.start()
    for i in range(parts):
        reads[i].wait()
        rows = buffer_ref[i]
        for to in range(SIDE):
            at = [(k * SIDE + to) * share for k in range(SIDE)]
            columns_ref[to, i * step : (i + 1) * step, :] = jnp.concatenate(
                [rows[:, a : a + share] for a in at], axis=1
            )


def columns_by_owner(flat, parts=4):
    rows, model = flat.shape
    return pl.pallas_call(
        columns_body,
        in_specs=[pl.BlockSpec(memory_space=pltpu.MemorySpace.HBM)],
        out_specs=VMEM,
        out_shape=jax.ShapeDtypeStruct((SIDE, rows, model // SIDE), flat.dtype),
        scratch_shapes=[
            pltpu.VMEM((parts, rows // parts, model), flat.dtype),
            pltpu.SemaphoreType.DMA((parts,)),
        ],
        interpret=INTERPRET,
        name="columns",
    )(flat)


def partial_body(tokens_ref, weights_ref, gates_ref, sent_ref):
    line, rows, _ = tokens_ref.shape
    owners, halves, sent_rows, width = sent_ref.shape
    ranges = line // halves
    positions = (sent_rows - gates_ref.shape[2]) // ranges
    prompts = rows // positions
    heads = owners // prompts
    for k in range(line):
        half, j = k // ranges, k % ranges
        part = jnp.dot(tokens_ref[k], weights_ref[...], preferred_element_type=jnp.float32)
        part = part.astype(sent_ref.dtype)
        for p in range(prompts):
            for h in range(heads):
                sent_ref[p * heads + h, half, j * positions : (j + 1) * positions, :] = part[
                    p * positions : (p + 1) * positions, h * width : (h + 1) * width
                ]
    sent_ref[:, :, ranges * positions :, :] = gates_ref[...]


def partial_projections(tokens, weights, gates, positions):
    owners, halves, extra, width = gates.shape
    sent_rows = tokens.shape[0] // halves * positions + extra
    return pl.pallas_call(
        partial_body,
        in_specs=[VMEM, VMEM, VMEM],
        out_specs=VMEM,
        out_shape=jax.ShapeDtypeStruct((owners, halves, sent_rows, width), tokens.dtype),
        interpret=INTERPRET,
        compiler_params=SMALL,
        name="partials",
    )(tokens, weights, gates)


def two_parts(values):
    high = lax.reduce_precision(values, 8, 7)
    return high.astype(jnp.bfloat16), (values - high).astype(jnp.bfloat16)


def best(left, right, dims=((1,), (0,))):
    return lax.dot_general(
        left, right, (dims, ((), ())), precision=BEST, preferred_element_type=jnp.float32
    )


def parts(x):
    high = x.astype(jnp.bfloat16)
    return high, (x - high.astype(jnp.float32)).astype(jnp.bfloat16)


def times(state, matrix):
    rows = state.shape[0]
    both = jnp.dot(
        jnp.concatenate(parts(state), axis=0), matrix, preferred_element_type=jnp.float32
    )
    return both[:rows] + both[rows:]


def near(left, right, dims=((1,), (0,))):
    (a, b), (c, d) = parts(left), parts(right)

    def dot(u, v):
        return lax.dot_general(u, v, (dims, ((), ())), preferred_element_type=jnp.float32)

    return dot(a, c) + (dot(a, d) + dot(b, c))


def silu(x):
    return x / (1.0 + jnp.exp(-x))


def ranges_body(half_ref, got_ref, sent_ref, kept_ref):
    line, _, width = got_ref.shape
    wide = width // 2
    ranges = line // 2
    positions = sent_ref.shape[0] // (ranges * 3)
    count = ranges * positions
    half = half_ref[0]
    sums = got_ref[0, :count, :].astype(jnp.float32)
    for k in range(1, line):
        sums = sums + got_ref[k, :count, :].astype(jnp.float32)
    keys = silu(sums[:, :wide])
    keys = keys * lax.rsqrt(jnp.sum(keys * keys, axis=-1, keepdims=True) + EPSILON)
    values = silu(sums[:, wide:])
    gates = got_ref[pl.ds(half * ranges, ranges), count:, :wide].astype(jnp.float32)
    beta = gates[:, 0, :] + gates[:, 1, :]
    fading = gates[:, 2, :] + gates[:, 3, :]
    up_to = lax.broadcasted_iota(jnp.int32, (wide, wide), 0) <= lax.broadcasted_iota(
        jnp.int32, (wide, wide), 1
    )
    sums_to = best(jnp.concatenate([beta, fading], axis=0), up_to.astype(jnp.float32))[ranges:]
    columns = jnp.concatenate([beta, sums_to], axis=0).T
    row = lax.broadcasted_iota(jnp.int32, (positions, positions), 0)
    column = lax.broadcasted_iota(jnp.int32, (positions, positions), 1)
    strict = row > column
    unit = (
        lax.broadcasted_iota(jnp.int32, (wide, wide), 0)
        == lax.broadcasted_iota(jnp.int32, (wide, wide), 1)
    ).astype(jnp.float32)
    powers, solved, tails, lasts = [], [], [], []
    for j in range(ranges):
        at = slice(j * positions, (j + 1) * positions)
        b = columns[:positions, j : j + 1]
        total = columns[:positions, ranges + j : ranges + j + 1]
        last = total[positions - 1 :, :]
        across = sums_to[j : j + 1, :positions]
        scaled = keys[at] * b
        inner = best(scaled, keys[at], ((1,), (1,)))
        spread = jnp.exp(jnp.where(strict, total - across, 0.0))
        powers.append(jnp.where(strict, inner * spread, 0.0))
        solved.append(jnp.concatenate([scaled * jnp.exp(total), values[at] * b], axis=1))
        tails.append(keys[at] * jnp.exp(last - total))
        lasts.append(jnp.exp(last))
    for j in range(ranges):
        solved[j] = solved[j] - best(powers[j], solved[j])
    reached = 2
    while reached < positions:
        for j in range(ranges):
            powers[j] = best(powers[j], powers[j])
        for j in range(ranges):
            solved[j] = solved[j] + best(powers[j], solved[j])
        reached *= 2
    so_far = None
    for j in range(ranges):
        moved = near(solved[j], tails[j], ((0,), (0,)))
        step = lasts[j] * unit - moved[:wide]
        if so_far is None:
            so_far = jnp.concatenate([step, moved[wide:]], axis=0)
        else:
            both = near(so_far, step)
            so_far = jnp.concatenate([both[:wide], both[wide:] + moved[wide:]], axis=0)
        out = so_far.astype(jnp.bfloat16)
        low, high = out[wide : wide + positions], out[wide + positions :]
        sent_ref[j * wide : (j + 1) * wide, :] = out[:wide]
        at = slice(ranges * wide + j * positions, ranges * wide + (j + 1) * positions)
        sent_ref[at, :] = jnp.where(half == 0, high, low)
        kept_ref[j * wide : (j + 1) * wide, :] = out[:wide]
        kept_ref[at, :] = jnp.where(half == 0, low, high)


def line_body(half_ref, kept_ref, other_ref, sent_ref):
    count, wide = kept_ref.shape
    ranges = 2 * count // (3 * wide)
    rows = wide // 2
    mine_first = half_ref[0] == 0
    step = slice((ranges - 1) * wide, ranges * wide)
    kept = jnp.concatenate([kept_ref[step, :], kept_ref[count - rows :, :]], axis=0)
    other = jnp.concatenate([other_ref[step, :], other_ref[count - rows :, :]], axis=0)
    first = jnp.where(mine_first, kept, other)
    second = jnp.where(mine_first, other, kept)
    both = jnp.dot(first, second[:wide], preferred_element_type=jnp.float32)
    added = both[wide:] + second[wide:].astype(jnp.float32)
    out = jnp.concatenate([both[:wide], added], axis=0).astype(jnp.bfloat16)
    for k in range(sent_ref.shape[0]):
        sent_ref[k] = out


def scan_body(place_ref, lines_ref, kept_ref, other_ref, sent_ref):
    lines, _, wide = lines_ref.shape
    rows = wide // 2
    ranges = sent_ref.shape[0] // 2
    z, mine_first = place_ref[0], place_ref[1] == 0
    state = lines_ref[0, wide:, :].astype(jnp.float32)
    entering = jnp.zeros_like(state)
    for k in range(1, lines):
        entering = jnp.where(z == k, state, entering)
        state = times(state, lines_ref[k, :wide, :]) + lines_ref[k, wide:, :].astype(jnp.float32)
    final = state.astype(jnp.bfloat16)
    state = entering
    for h in range(2):
        begin = state
        for j in range(ranges):
            step = slice(j * wide, (j + 1) * wide)
            extra = slice(ranges * wide + j * rows, ranges * wide + (j + 1) * rows)
            use_kept = mine_first if h == 0 else jnp.logical_not(mine_first)
            matrix = jnp.where(use_kept, kept_ref[step, :], other_ref[step, :])
            added = jnp.where(use_kept, kept_ref[extra, :], other_ref[extra, :])
            state = times(begin, matrix) + added.astype(jnp.float32)
            sent_ref[h * ranges + j, :rows, :] = state.astype(jnp.bfloat16)
            sent_ref[h * ranges + j, rows:, :] = final


def read_body(
    strength_ref,
    back_ref,
    probe_ref,
    address_ref,
    content_ref,
    outgate_ref,
    gain_ref,
    readout_ref,
    sent_ref,
):
    wide = back_ref.shape[2]
    rows = wide // 2
    prompts, width = probe_ref.shape
    heads = width // wide
    each = [(p, h) for p in range(prompts) for h in range(heads)]

    def gathered(ref):
        wanted = [ref[p : p + 1, h * wide : (h + 1) * wide] for p, h in each]
        return jnp.concatenate(wanted, axis=0).astype(jnp.float32)

    query = silu(gathered(probe_ref))
    key = silu(gathered(address_ref))
    key = key * lax.rsqrt(jnp.sum(key * key, axis=-1, keepdims=True) + EPSILON)
    value = silu(gathered(content_ref))
    strength = jnp.concatenate(
        [jnp.full((1, 1), strength_ref[p, h], jnp.float32) for p, h in each], axis=0
    )
    strength = 1.0 / (1.0 + jnp.exp(-strength))
    pair = jnp.concatenate([key, query], axis=0)
    recalled, probed = [], []
    for n in range(len(each)):
        state = jnp.concatenate([back_ref[2 * n, rows:, :], back_ref[2 * n + 1, rows:, :]], axis=0)
        found = best(pair, state.astype(jnp.float32), ((1,), (1,)))
        recalled.append(found[n : n + 1])
        probed.append(found[len(each) + n : len(each) + n + 1])
    along = jnp.sum(key * query, axis=-1, keepdims=True)
    out = jnp.concatenate(probed, axis=0) + strength * along * (
        value - jnp.concatenate(recalled, axis=0)
    )
    out = out * lax.rsqrt(jnp.mean(out * out, axis=-1, keepdims=True) + EPSILON)
    read = out * gain_ref[...] * silu(gathered(outgate_ref))
    rows_of = [
        jnp.concatenate([read[p * heads + h :][:1] for h in range(heads)], axis=1)
        for p in range(prompts)
    ]
    heads_read = jnp.concatenate(rows_of, axis=0).astype(jnp.bfloat16)
    terms = jnp.dot(heads_read, readout_ref[...], preferred_element_type=jnp.float32)
    for k in range(sent_ref.shape[0]):
        sent_ref[k] = terms.astype(jnp.bfloat16)


SMEM = pl.BlockSpec(memory_space=pltpu.SMEM)


def local(body, name, shapes, *operands):
    out = [jax.ShapeDtypeStruct(shape, jnp.bfloat16) for shape in shapes]
    return pl.pallas_call(
        body,
        in_specs=[SMEM] + [VMEM] * (len(operands) - 1),
        out_specs=[VMEM] * len(out),
        out_shape=out,
        interpret=INTERPRET,
        compiler_params=SMALL,
        name=name,
    )(*operands)


def per_device(
    tokens,
    address_projection,
    content_projection,
    strength_projection,
    fading_driver_projection,
    strength_offset,
    fading_speed,
    added_fading,
    probe,
    address,
    content,
    outgate,
    strength_raw,
    gain,
    readout_projection,
):
    prompts, positions, model = tokens.shape
    heads = fading_speed.shape[0]
    rows = prompts * positions
    share = model // (SIDE * SIDE)
    z, y, tp = lax.axis_index(Z), lax.axis_index("y"), lax.axis_index("tp")
    half = SIDE // 2
    my_half = y % 2

    weights = jnp.concatenate(
        [
            part[:, head * WIDTH : (head + 1) * WIDTH]
            for head in range(heads)
            for part in (address_projection, content_projection)
        ],
        axis=1,
    )
    flat = tokens.reshape(rows, model)
    columns = columns_by_owner(flat)
    line_tokens = exchange(columns, "y")
    beside = lax.ppermute(weights, "zl", [(0, 1), (1, 0)])
    even = lax.axis_index("zl") == 0
    both = [jnp.where(even, weights, beside), jnp.where(even, beside, weights)]
    line_weights = lax.all_gather(jnp.concatenate(both), "zh", axis=0, tiled=True)

    drivers = jnp.concatenate([strength_projection, fading_driver_projection], axis=1)
    logits = jnp.dot(flat, drivers, preferred_element_type=jnp.float32).astype(jnp.bfloat16)
    logits = logits.astype(jnp.float32).reshape(prompts, positions, 2, -1)
    mine = lax.dynamic_slice_in_dim(logits, tp * heads, heads, 3)
    beta = jax.nn.sigmoid(mine[:, :, 0] + strength_offset)
    fading = added_fading - fading_speed * jax.nn.softplus(mine[:, :, 1])
    gates = jnp.stack([*two_parts(beta), *two_parts(fading)])
    gates = jnp.pad(
        gates.transpose(1, 3, 0, 2), ((0, 0), (0, 0), (0, 4), (0, 2 * WIDTH - positions))
    )

    gates = jnp.broadcast_to(gates[:, :, None], (prompts, heads, 2, *gates.shape[2:]))
    sent = partial_projections(
        line_tokens,
        line_weights,
        gates.reshape(prompts * heads, *gates.shape[2:]),
        positions,
    )
    got = exchange(sent.reshape(SIDE, *sent.shape[2:]), "y")

    side = my_half.astype(jnp.int32).reshape(1)
    size = (half * (WIDTH + WIDTH // 2), WIDTH)
    given, kept = local(ranges_body, "ranges", [size, size], side, got)
    other = lax.ppermute(given, "y", [(i, i ^ 1) for i in range(SIDE)])
    (line,) = local(line_body, "line", [(SIDE, WIDTH + WIDTH // 2, WIDTH)], side, kept, other)
    lines = exchange(line, Z)
    place = jnp.stack([z, my_half]).astype(jnp.int32)
    (home,) = local(scan_body, "scan", [(SIDE, WIDTH, WIDTH)], place, lines, kept, other)

    back = exchange(home, "y")
    (terms,) = local(
        read_body,
        "read",
        [(lax.axis_size("tp"), prompts, readout_projection.shape[1])],
        strength_raw,
        back,
        probe,
        address,
        content,
        outgate,
        gain.reshape(1, WIDTH),
        readout_projection,
    )
    mixed = exchange(terms, "tp").astype(jnp.float32).sum(axis=0)
    states = back.reshape(prompts, heads, 2, 2, WIDTH // 2, WIDTH).transpose(3, 0, 1, 5, 2, 4)
    boundary, state_cache = states.reshape(2, prompts, heads, WIDTH, WIDTH)
    return state_cache, mixed.astype(jnp.bfloat16), boundary[:, None]


def solution(mesh):
    finer = Mesh(mesh.devices.reshape(SIDE // 2, 2, SIDE, mesh.shape["tp"]), (*SP, "tp"))
    return jax.shard_map(
        per_device,
        mesh=finer,
        in_specs=(
            P(None, SP, None),
            P(SP, "tp"),
            P(SP, "tp"),
            P(),
            P(),
            P("tp"),
            P("tp"),
            P(None, SP, "tp"),
            P(None, "tp"),
            P(None, "tp"),
            P(None, "tp"),
            P(None, "tp"),
            P(None, "tp"),
            P(),
            P("tp", SP),
        ),
        out_specs=(P(None, "tp", None, None), P(None, SP), P(None, SP, "tp", None, None)),
        check_vma=False,
    )
```

```python
import jax
import jax.numpy as jnp
from jax import lax
from jax.experimental import pallas as pl
from jax.experimental.pallas import tpu as pltpu
from jax.sharding import Mesh
from jax.sharding import PartitionSpec as P

WIDTH = 128
SIDE = 8
EPSILON = 1e-06
BEST = lax.Precision.HIGHEST
Z = ("zh", "zl")
SP = (*Z, "y")
INTERPRET = False
VMEM = pl.BlockSpec(memory_space=pltpu.VMEM)
SMALL = pltpu.CompilerParams(vmem_limit_bytes=16 * 1024 * 1024)


def exchange(messages, axis):
    return lax.all_to_all(messages, axis, split_axis=0, concat_axis=0, tiled=True)


def columns_body(prompt_ref, tokens_ref, columns_ref, buffer_ref, arrived):
    parts, step, model = buffer_ref.shape
    share = model // (SIDE * SIDE)
    reads = [
        pltpu.make_async_copy(
            tokens_ref.at[prompt_ref[0], i * step : (i + 1) * step, :],
            buffer_ref.at[i],
            arrived.at[i],
        )
        for i in range(parts)
    ]
    for read in reads:
        read.start()
    for i in range(parts):
        reads[i].wait()
        rows = buffer_ref[i]
        for to in range(SIDE):
            at = [(k * SIDE + to) * share for k in range(SIDE)]
            columns_ref[to, i * step : (i + 1) * step, :] = jnp.concatenate(
                [rows[:, a : a + share] for a in at], axis=1
            )


def columns_by_owner(prompt, tokens, parts=2):
    _, rows, model = tokens.shape
    return pl.pallas_call(
        columns_body,
        in_specs=[
            pl.BlockSpec(memory_space=pltpu.SMEM),
            pl.BlockSpec(memory_space=pltpu.MemorySpace.HBM),
        ],
        out_specs=VMEM,
        out_shape=jax.ShapeDtypeStruct((SIDE, rows, model // SIDE), tokens.dtype),
        scratch_shapes=[
            pltpu.VMEM((parts, rows // parts, model), tokens.dtype),
            pltpu.SemaphoreType.DMA((parts,)),
        ],
        interpret=INTERPRET,
        name="columns",
    )(prompt, tokens)


def partial_body(prompt_ref, mine_ref, other_ref, weights_ref, gates_ref, sent_ref):
    line, positions, share = mine_ref.shape
    prompts, heads, halves, _, width = sent_ref.shape
    ranges = line // halves
    for tokens_ref, p in ((mine_ref, prompt_ref[0]), (other_ref, 1 - prompt_ref[0])):
        for half in range(halves):
            rows = tokens_ref[half * ranges : (half + 1) * ranges].reshape(-1, share)
            part = jnp.dot(rows, weights_ref[...], preferred_element_type=jnp.float32)
            part = part.astype(sent_ref.dtype)
            for h in range(heads):
                sent_ref[p, h, half, : ranges * positions, :] = part[:, h * width : (h + 1) * width]
    sent_ref[:, :, :, ranges * positions :, :] = gates_ref[...]


def partial_projections(prompt, mine, other, weights, gates):
    prompts, heads, halves, extra, width = gates.shape
    line, positions, _ = mine.shape
    sent_rows = line // halves * positions + extra
    return pl.pallas_call(
        partial_body,
        in_specs=[pl.BlockSpec(memory_space=pltpu.SMEM), VMEM, VMEM, VMEM, VMEM],
        out_specs=VMEM,
        out_shape=jax.ShapeDtypeStruct((prompts, heads, halves, sent_rows, width), mine.dtype),
        interpret=INTERPRET,
        compiler_params=SMALL,
        name="partials",
    )(prompt, mine, other, weights, gates)


def two_parts(values):
    high = lax.reduce_precision(values, 8, 7)
    return high.astype(jnp.bfloat16), (values - high).astype(jnp.bfloat16)


def best(left, right, dims=((1,), (0,))):
    return lax.dot_general(
        left, right, (dims, ((), ())), precision=BEST, preferred_element_type=jnp.float32
    )


def parts(x):
    high = x.astype(jnp.bfloat16)
    return high, (x - high.astype(jnp.float32)).astype(jnp.bfloat16)


def times(state, matrix):
    rows = state.shape[0]
    both = jnp.dot(
        jnp.concatenate(parts(state), axis=0), matrix, preferred_element_type=jnp.float32
    )
    return both[:rows] + both[rows:]


def near(left, right, dims=((1,), (0,))):
    (a, b), (c, d) = parts(left), parts(right)

    def dot(u, v):
        return lax.dot_general(u, v, (dims, ((), ())), preferred_element_type=jnp.float32)

    return dot(a, c) + (dot(a, d) + dot(b, c))


def silu(x):
    return x / (1.0 + jnp.exp(-x))


def ranges_body(half_ref, got_ref, sent_ref, kept_ref):
    line, _, width = got_ref.shape
    wide = width // 2
    ranges = line // 2
    positions = sent_ref.shape[0] // (ranges * 3)
    count = ranges * positions
    half = half_ref[0]
    sums = got_ref[0, :count, :].astype(jnp.float32)
    for k in range(1, line):
        sums = sums + got_ref[k, :count, :].astype(jnp.float32)
    keys = silu(sums[:, :wide])
    keys = keys * lax.rsqrt(jnp.sum(keys * keys, axis=-1, keepdims=True) + EPSILON)
    values = silu(sums[:, wide:])
    gates = got_ref[pl.ds(half * ranges, ranges), count:, :wide].astype(jnp.float32)
    beta = gates[:, 0, :] + gates[:, 1, :]
    fading = gates[:, 2, :] + gates[:, 3, :]
    up_to = lax.broadcasted_iota(jnp.int32, (wide, wide), 0) <= lax.broadcasted_iota(
        jnp.int32, (wide, wide), 1
    )
    sums_to = best(jnp.concatenate([beta, fading], axis=0), up_to.astype(jnp.float32))[ranges:]
    columns = jnp.concatenate([beta, sums_to], axis=0).T
    row = lax.broadcasted_iota(jnp.int32, (positions, positions), 0)
    column = lax.broadcasted_iota(jnp.int32, (positions, positions), 1)
    strict = row > column
    unit = (
        lax.broadcasted_iota(jnp.int32, (wide, wide), 0)
        == lax.broadcasted_iota(jnp.int32, (wide, wide), 1)
    ).astype(jnp.float32)
    powers, solved, tails, lasts = [], [], [], []
    for j in range(ranges):
        at = slice(j * positions, (j + 1) * positions)
        b = columns[:positions, j : j + 1]
        total = columns[:positions, ranges + j : ranges + j + 1]
        last = total[positions - 1 :, :]
        across = sums_to[j : j + 1, :positions]
        scaled = keys[at] * b
        inner = best(scaled, keys[at], ((1,), (1,)))
        spread = jnp.exp(jnp.where(strict, total - across, 0.0))
        powers.append(jnp.where(strict, inner * spread, 0.0))
        solved.append(jnp.concatenate([scaled * jnp.exp(total), values[at] * b], axis=1))
        tails.append(keys[at] * jnp.exp(last - total))
        lasts.append(jnp.exp(last))
    for j in range(ranges):
        solved[j] = solved[j] - best(powers[j], solved[j])
    reached = 2
    while reached < positions:
        for j in range(ranges):
            powers[j] = best(powers[j], powers[j])
        for j in range(ranges):
            solved[j] = solved[j] + best(powers[j], solved[j])
        reached *= 2
    so_far = None
    for j in range(ranges):
        moved = near(solved[j], tails[j], ((0,), (0,)))
        step = lasts[j] * unit - moved[:wide]
        if so_far is None:
            so_far = jnp.concatenate([step, moved[wide:]], axis=0)
        else:
            both = near(so_far, step)
            so_far = jnp.concatenate([both[:wide], both[wide:] + moved[wide:]], axis=0)
        out = so_far.astype(jnp.bfloat16)
        low, high = out[wide : wide + positions], out[wide + positions :]
        sent_ref[j * wide : (j + 1) * wide, :] = out[:wide]
        at = slice(ranges * wide + j * positions, ranges * wide + (j + 1) * positions)
        sent_ref[at, :] = jnp.where(half == 0, high, low)
        kept_ref[j * wide : (j + 1) * wide, :] = out[:wide]
        kept_ref[at, :] = jnp.where(half == 0, low, high)


def line_body(half_ref, kept_ref, other_ref, sent_ref):
    count, wide = kept_ref.shape
    ranges = 2 * count // (3 * wide)
    rows = wide // 2
    mine_first = half_ref[0] == 0
    step = slice((ranges - 1) * wide, ranges * wide)
    kept = jnp.concatenate([kept_ref[step, :], kept_ref[count - rows :, :]], axis=0)
    other = jnp.concatenate([other_ref[step, :], other_ref[count - rows :, :]], axis=0)
    first = jnp.where(mine_first, kept, other)
    second = jnp.where(mine_first, other, kept)
    both = jnp.dot(first, second[:wide], preferred_element_type=jnp.float32)
    added = both[wide:] + second[wide:].astype(jnp.float32)
    out = jnp.concatenate([both[:wide], added], axis=0).astype(jnp.bfloat16)
    for k in range(sent_ref.shape[0]):
        sent_ref[k] = out


def scan_body(place_ref, lines_ref, kept_ref, other_ref, sent_ref):
    lines, _, wide = lines_ref.shape
    rows = wide // 2
    ranges = sent_ref.shape[0] // 2
    z, mine_first = place_ref[0], place_ref[1] == 0
    state = lines_ref[0, wide:, :].astype(jnp.float32)
    entering = jnp.zeros_like(state)
    for k in range(1, lines):
        entering = jnp.where(z == k, state, entering)
        state = times(state, lines_ref[k, :wide, :]) + lines_ref[k, wide:, :].astype(jnp.float32)
    final = state.astype(jnp.bfloat16)
    state = entering
    for h in range(2):
        begin = state
        for j in range(ranges):
            step = slice(j * wide, (j + 1) * wide)
            extra = slice(ranges * wide + j * rows, ranges * wide + (j + 1) * rows)
            use_kept = mine_first if h == 0 else jnp.logical_not(mine_first)
            matrix = jnp.where(use_kept, kept_ref[step, :], other_ref[step, :])
            added = jnp.where(use_kept, kept_ref[extra, :], other_ref[extra, :])
            state = times(begin, matrix) + added.astype(jnp.float32)
            sent_ref[h * ranges + j, :rows, :] = state.astype(jnp.bfloat16)
            sent_ref[h * ranges + j, rows:, :] = final


def read_body(
    strength_ref,
    back_ref,
    probe_ref,
    address_ref,
    content_ref,
    outgate_ref,
    gain_ref,
    readout_ref,
    sent_ref,
):
    wide = back_ref.shape[2]
    rows = wide // 2
    prompts, width = probe_ref.shape
    heads = width // wide
    each = [(p, h) for p in range(prompts) for h in range(heads)]

    def gathered(ref):
        wanted = [ref[p : p + 1, h * wide : (h + 1) * wide] for p, h in each]
        return jnp.concatenate(wanted, axis=0).astype(jnp.float32)

    query = silu(gathered(probe_ref))
    key = silu(gathered(address_ref))
    key = key * lax.rsqrt(jnp.sum(key * key, axis=-1, keepdims=True) + EPSILON)
    value = silu(gathered(content_ref))
    strength = jnp.concatenate(
        [jnp.full((1, 1), strength_ref[p, h], jnp.float32) for p, h in each], axis=0
    )
    strength = 1.0 / (1.0 + jnp.exp(-strength))
    pair = jnp.concatenate([key, query], axis=0)
    recalled, probed = [], []
    for n in range(len(each)):
        state = jnp.concatenate([back_ref[2 * n, rows:, :], back_ref[2 * n + 1, rows:, :]], axis=0)
        found = best(pair, state.astype(jnp.float32), ((1,), (1,)))
        recalled.append(found[n : n + 1])
        probed.append(found[len(each) + n : len(each) + n + 1])
    along = jnp.sum(key * query, axis=-1, keepdims=True)
    out = jnp.concatenate(probed, axis=0) + strength * along * (
        value - jnp.concatenate(recalled, axis=0)
    )
    out = out * lax.rsqrt(jnp.mean(out * out, axis=-1, keepdims=True) + EPSILON)
    read = out * gain_ref[...] * silu(gathered(outgate_ref))
    rows_of = [
        jnp.concatenate([read[p * heads + h :][:1] for h in range(heads)], axis=1)
        for p in range(prompts)
    ]
    heads_read = jnp.concatenate(rows_of, axis=0).astype(jnp.bfloat16)
    terms = jnp.dot(heads_read, readout_ref[...], preferred_element_type=jnp.float32)
    for k in range(sent_ref.shape[0]):
        sent_ref[k] = terms.astype(jnp.bfloat16)


SMEM = pl.BlockSpec(memory_space=pltpu.SMEM)


def local(body, name, shapes, *operands):
    out = [jax.ShapeDtypeStruct(shape, jnp.bfloat16) for shape in shapes]
    return pl.pallas_call(
        body,
        in_specs=[SMEM] + [VMEM] * (len(operands) - 1),
        out_specs=[VMEM] * len(out),
        out_shape=out,
        interpret=INTERPRET,
        compiler_params=SMALL,
        name=name,
    )(*operands)


def per_device(
    tokens,
    address_projection,
    content_projection,
    strength_projection,
    fading_driver_projection,
    strength_offset,
    fading_speed,
    added_fading,
    probe,
    address,
    content,
    outgate,
    strength_raw,
    gain,
    readout_projection,
):
    prompts, positions, model = tokens.shape
    heads = fading_speed.shape[0]
    rows = prompts * positions
    share = model // (SIDE * SIDE)
    z, y, tp = lax.axis_index(Z), lax.axis_index("y"), lax.axis_index("tp")
    half = SIDE // 2
    my_half = y % 2

    weights = jnp.concatenate(
        [
            part[:, head * WIDTH : (head + 1) * WIDTH]
            for head in range(heads)
            for part in (address_projection, content_projection)
        ],
        axis=1,
    )
    flat = tokens.reshape(rows, model)
    prompt = (tp % 2).astype(jnp.int32).reshape(1)
    mine = exchange(columns_by_owner(prompt, tokens), "y")
    beside = lax.ppermute(weights, "zl", [(0, 1), (1, 0)])
    even = lax.axis_index("zl") == 0
    both = [jnp.where(even, weights, beside), jnp.where(even, beside, weights)]
    line_weights = lax.all_gather(jnp.concatenate(both), "zh", axis=0, tiled=True)
    mine, line_weights = lax.optimization_barrier((mine, line_weights))
    other = lax.ppermute(mine, "tp", [(i, i ^ 1) for i in range(lax.axis_size("tp"))])

    drivers = jnp.concatenate([strength_projection, fading_driver_projection], axis=1)
    logits = jnp.dot(flat, drivers, preferred_element_type=jnp.float32).astype(jnp.bfloat16)
    logits = logits.astype(jnp.float32).reshape(prompts, positions, 2, -1)
    own = lax.dynamic_slice_in_dim(logits, tp * heads, heads, 3)
    beta = jax.nn.sigmoid(own[:, :, 0] + strength_offset)
    fading = added_fading - fading_speed * jax.nn.softplus(own[:, :, 1])
    gates = jnp.stack([*two_parts(beta), *two_parts(fading)])
    gates = jnp.pad(
        gates.transpose(1, 3, 0, 2), ((0, 0), (0, 0), (0, 4), (0, 2 * WIDTH - positions))
    )

    gates = jnp.broadcast_to(gates[:, :, None], (prompts, heads, 2, *gates.shape[2:]))
    sent = partial_projections(prompt, mine, other, line_weights, gates)
    got = exchange(sent.reshape(SIDE, *sent.shape[3:]), "y")

    side = my_half.astype(jnp.int32).reshape(1)
    size = (half * (WIDTH + WIDTH // 2), WIDTH)
    given, kept = local(ranges_body, "ranges", [size, size], side, got)
    other = lax.ppermute(given, "y", [(i, i ^ 1) for i in range(SIDE)])
    (line,) = local(line_body, "line", [(SIDE, WIDTH + WIDTH // 2, WIDTH)], side, kept, other)
    lines = exchange(line, Z)
    place = jnp.stack([z, my_half]).astype(jnp.int32)
    (home,) = local(scan_body, "scan", [(SIDE, WIDTH, WIDTH)], place, lines, kept, other)

    back = exchange(home, "y")
    (terms,) = local(
        read_body,
        "read",
        [(lax.axis_size("tp"), prompts, readout_projection.shape[1])],
        strength_raw,
        back,
        probe,
        address,
        content,
        outgate,
        gain.reshape(1, WIDTH),
        readout_projection,
    )
    mixed = exchange(terms, "tp").astype(jnp.float32).sum(axis=0)
    states = back.reshape(prompts, heads, 2, 2, WIDTH // 2, WIDTH).transpose(3, 0, 1, 5, 2, 4)
    boundary, state_cache = states.reshape(2, prompts, heads, WIDTH, WIDTH)
    return state_cache, mixed.astype(jnp.bfloat16), boundary[:, None]


def solution(mesh):
    finer = Mesh(mesh.devices.reshape(SIDE // 2, 2, SIDE, mesh.shape["tp"]), (*SP, "tp"))
    return jax.shard_map(
        per_device,
        mesh=finer,
        in_specs=(
            P(None, SP, None),
            P(SP, "tp"),
            P(SP, "tp"),
            P(),
            P(),
            P("tp"),
            P("tp"),
            P(None, SP, "tp"),
            P(None, "tp"),
            P(None, "tp"),
            P(None, "tp"),
            P(None, "tp"),
            P(None, "tp"),
            P(),
            P("tp", SP),
        ),
        out_specs=(P(None, "tp", None, None), P(None, SP), P(None, SP, "tp", None, None)),
        check_vma=False,
    )
```

```python
import jax
import jax.numpy as jnp
from jax import lax
from jax.experimental import pallas as pl
from jax.experimental.pallas import tpu as pltpu
from jax.sharding import Mesh
from jax.sharding import PartitionSpec as P

WIDTH = 128
SIDE = 8
EPSILON = 1e-06
BEST = lax.Precision.HIGHEST
SP = ("z", "y")
INTERPRET = False
VMEM = pl.BlockSpec(memory_space=pltpu.VMEM)
SMALL = pltpu.CompilerParams(vmem_limit_bytes=16 * 1024 * 1024)


def exchange(messages, axis):
    return lax.all_to_all(messages, axis, split_axis=0, concat_axis=0, tiled=True)


def columns_body(tokens_ref, columns_ref, buffer_ref, arrived):
    parts, step, model = buffer_ref.shape
    share = model // (SIDE * SIDE)
    reads = [
        pltpu.make_async_copy(
            tokens_ref.at[i * step : (i + 1) * step, :], buffer_ref.at[i], arrived.at[i]
        )
        for i in range(parts)
    ]
    for read in reads:
        read.start()
    for i in range(parts):
        reads[i].wait()
        rows = buffer_ref[i]
        for to in range(SIDE):
            at = [(k * SIDE + to) * share for k in range(SIDE)]
            columns_ref[to, i * step : (i + 1) * step, :] = jnp.concatenate(
                [rows[:, a : a + share] for a in at], axis=1
            )


def columns_by_owner(flat, parts=4):
    rows, model = flat.shape
    return pl.pallas_call(
        columns_body,
        in_specs=[pl.BlockSpec(memory_space=pltpu.MemorySpace.HBM)],
        out_specs=VMEM,
        out_shape=jax.ShapeDtypeStruct((SIDE, rows, model // SIDE), flat.dtype),
        scratch_shapes=[
            pltpu.VMEM((parts, rows // parts, model), flat.dtype),
            pltpu.SemaphoreType.DMA((parts,)),
        ],
        interpret=INTERPRET,
        name="columns",
    )(flat)


def partial_body(tokens_ref, weights_ref, gates_ref, sent_ref):
    line, rows, _ = tokens_ref.shape
    owners, halves, sent_rows, width = sent_ref.shape
    ranges = line // halves
    positions = (sent_rows - gates_ref.shape[2]) // ranges
    prompts = rows // positions
    heads = owners // prompts
    for k in range(line):
        half, j = k // ranges, k % ranges
        part = jnp.dot(tokens_ref[k], weights_ref[...], preferred_element_type=jnp.float32)
        part = part.astype(sent_ref.dtype)
        for p in range(prompts):
            for h in range(heads):
                sent_ref[p * heads + h, half, j * positions : (j + 1) * positions, :] = part[
                    p * positions : (p + 1) * positions, h * width : (h + 1) * width
                ]
    sent_ref[:, :, ranges * positions :, :] = gates_ref[...]


def partial_projections(tokens, weights, gates, positions):
    owners, halves, extra, width = gates.shape
    sent_rows = tokens.shape[0] // halves * positions + extra
    return pl.pallas_call(
        partial_body,
        in_specs=[VMEM, VMEM, VMEM],
        out_specs=VMEM,
        out_shape=jax.ShapeDtypeStruct((owners, halves, sent_rows, width), tokens.dtype),
        interpret=INTERPRET,
        compiler_params=SMALL,
        name="partials",
    )(tokens, weights, gates)


def two_parts(values):
    high = lax.reduce_precision(values, 8, 7)
    return high.astype(jnp.bfloat16), (values - high).astype(jnp.bfloat16)


def best(left, right, dims=((1,), (0,))):
    return lax.dot_general(
        left, right, (dims, ((), ())), precision=BEST, preferred_element_type=jnp.float32
    )


def parts(x):
    high = x.astype(jnp.bfloat16)
    return high, (x - high.astype(jnp.float32)).astype(jnp.bfloat16)


def times(state, matrix):
    rows = state.shape[0]
    both = jnp.dot(
        jnp.concatenate(parts(state), axis=0), matrix, preferred_element_type=jnp.float32
    )
    return both[:rows] + both[rows:]


def near(left, right, dims=((1,), (0,))):
    (a, b), (c, d) = parts(left), parts(right)

    def dot(u, v):
        return lax.dot_general(u, v, (dims, ((), ())), preferred_element_type=jnp.float32)

    return dot(a, c) + (dot(a, d) + dot(b, c))


def silu(x):
    return x / (1.0 + jnp.exp(-x))


def ranges_body(half_ref, got_ref, sent_ref, kept_ref):
    line, _, width = got_ref.shape
    wide = width // 2
    ranges = line // 2
    positions = sent_ref.shape[0] // (ranges * 3)
    count = ranges * positions
    half = half_ref[0]
    sums = got_ref[0, :count, :].astype(jnp.float32)
    for k in range(1, line):
        sums = sums + got_ref[k, :count, :].astype(jnp.float32)
    keys = silu(sums[:, :wide])
    keys = keys * lax.rsqrt(jnp.sum(keys * keys, axis=-1, keepdims=True) + EPSILON)
    values = silu(sums[:, wide:])
    gates = got_ref[pl.ds(half * ranges, ranges), count:, :wide].astype(jnp.float32)
    beta = gates[:, 0, :] + gates[:, 1, :]
    fading = gates[:, 2, :] + gates[:, 3, :]
    up_to = lax.broadcasted_iota(jnp.int32, (wide, wide), 0) <= lax.broadcasted_iota(
        jnp.int32, (wide, wide), 1
    )
    sums_to = best(jnp.concatenate([beta, fading], axis=0), up_to.astype(jnp.float32))[ranges:]
    columns = jnp.concatenate([beta, sums_to], axis=0).T
    row = lax.broadcasted_iota(jnp.int32, (positions, positions), 0)
    column = lax.broadcasted_iota(jnp.int32, (positions, positions), 1)
    strict = row > column
    unit = (
        lax.broadcasted_iota(jnp.int32, (wide, wide), 0)
        == lax.broadcasted_iota(jnp.int32, (wide, wide), 1)
    ).astype(jnp.float32)
    powers, solved, tails, lasts = [], [], [], []
    for j in range(ranges):
        at = slice(j * positions, (j + 1) * positions)
        b = columns[:positions, j : j + 1]
        total = columns[:positions, ranges + j : ranges + j + 1]
        last = total[positions - 1 :, :]
        across = sums_to[j : j + 1, :positions]
        scaled = keys[at] * b
        inner = best(scaled, keys[at], ((1,), (1,)))
        spread = jnp.exp(jnp.where(strict, total - across, 0.0))
        powers.append(jnp.where(strict, inner * spread, 0.0))
        solved.append(jnp.concatenate([scaled * jnp.exp(total), values[at] * b], axis=1))
        tails.append(keys[at] * jnp.exp(last - total))
        lasts.append(jnp.exp(last))
    for j in range(ranges):
        solved[j] = solved[j] - best(powers[j], solved[j])
    reached = 2
    while reached < positions:
        for j in range(ranges):
            powers[j] = best(powers[j], powers[j])
        for j in range(ranges):
            solved[j] = solved[j] + best(powers[j], solved[j])
        reached *= 2
    so_far = None
    for j in range(ranges):
        moved = near(solved[j], tails[j], ((0,), (0,)))
        step = lasts[j] * unit - moved[:wide]
        if so_far is None:
            so_far = jnp.concatenate([step, moved[wide:]], axis=0)
        else:
            both = near(so_far, step)
            so_far = jnp.concatenate([both[:wide], both[wide:] + moved[wide:]], axis=0)
        out = so_far.astype(jnp.bfloat16)
        low, high = out[wide : wide + positions], out[wide + positions :]
        sent_ref[j * wide : (j + 1) * wide, :] = out[:wide]
        at = slice(ranges * wide + j * positions, ranges * wide + (j + 1) * positions)
        sent_ref[at, :] = jnp.where(half == 0, high, low)
        kept_ref[j * wide : (j + 1) * wide, :] = out[:wide]
        kept_ref[at, :] = jnp.where(half == 0, low, high)


def line_body(half_ref, kept_ref, other_ref, sent_ref):
    count, wide = kept_ref.shape
    ranges = 2 * count // (3 * wide)
    rows = wide // 2
    mine_first = half_ref[0] == 0
    step = slice((ranges - 1) * wide, ranges * wide)
    kept = jnp.concatenate([kept_ref[step, :], kept_ref[count - rows :, :]], axis=0)
    other = jnp.concatenate([other_ref[step, :], other_ref[count - rows :, :]], axis=0)
    first = jnp.where(mine_first, kept, other)
    second = jnp.where(mine_first, other, kept)
    both = jnp.dot(first, second[:wide], preferred_element_type=jnp.float32)
    added = both[wide:] + second[wide:].astype(jnp.float32)
    out = jnp.concatenate([both[:wide], added], axis=0).astype(jnp.bfloat16)
    for k in range(sent_ref.shape[0]):
        sent_ref[k] = out


def scan_body(place_ref, lines_ref, kept_ref, other_ref, sent_ref):
    lines, _, wide = lines_ref.shape
    rows = wide // 2
    ranges = sent_ref.shape[0] // 2
    z, mine_first = place_ref[0], place_ref[1] == 0
    after, pairs = [], []
    for k in range(0, lines, 2):
        both = jnp.dot(
            lines_ref[k], lines_ref[k + 1, :wide, :], preferred_element_type=jnp.float32
        )
        added = both[wide:] + lines_ref[k + 1, wide:, :].astype(jnp.float32)
        pairs.append((parts(both[:wide]), added))
    state = jnp.zeros((rows, wide), jnp.float32)
    for k, ((high, low), added) in enumerate(pairs):
        after.append(state)
        if k:
            ours = jnp.concatenate(parts(state), axis=0)
            found = jnp.dot(ours, high, preferred_element_type=jnp.float32)
            found = found[:rows] + found[rows:]
            state = found + jnp.dot(ours[:rows], low, preferred_element_type=jnp.float32) + added
        else:
            state = added
    begin = after[0]
    for k in range(1, len(after)):
        begin = jnp.where(z // 2 == k, after[k], begin)
    before = lines_ref[(z // 2) * 2]
    stepped = times(begin, before[:wide]) + before[wide:].astype(jnp.float32)
    entering = jnp.where(z % 2 == 0, begin, stepped)
    final = state.astype(jnp.bfloat16)
    state = entering
    for h in range(2):
        begin = state
        for j in range(ranges):
            step = slice(j * wide, (j + 1) * wide)
            extra = slice(ranges * wide + j * rows, ranges * wide + (j + 1) * rows)
            use_kept = mine_first if h == 0 else jnp.logical_not(mine_first)
            matrix = jnp.where(use_kept, kept_ref[step, :], other_ref[step, :])
            added = jnp.where(use_kept, kept_ref[extra, :], other_ref[extra, :])
            state = times(begin, matrix) + added.astype(jnp.float32)
            sent_ref[h * ranges + j, :rows, :] = state.astype(jnp.bfloat16)
            sent_ref[h * ranges + j, rows:, :] = final


def first_step_body(
    strength_ref, probe_ref, address_ref, content_ref, outgate_ref, gain_ref, rows_ref
):
    prompts, width = probe_ref.shape
    wide = gain_ref.shape[1]
    each = [(p, h) for p in range(prompts) for h in range(width // wide)]
    count = len(each)

    def gathered(ref):
        wanted = [ref[p : p + 1, h * wide : (h + 1) * wide] for p, h in each]
        return jnp.concatenate(wanted, axis=0).astype(jnp.float32)

    query = silu(gathered(probe_ref))
    key = silu(gathered(address_ref))
    key = key * lax.rsqrt(jnp.sum(key * key, axis=-1, keepdims=True) + EPSILON)
    strength = jnp.concatenate(
        [jnp.full((1, 1), strength_ref[p, h], jnp.float32) for p, h in each], axis=0
    )
    strength = 1.0 / (1.0 + jnp.exp(-strength))
    along = jnp.sum(key * query, axis=-1, keepdims=True)
    rest = jnp.concatenate([key, query], axis=0)
    for k in range(3):
        part = rest.astype(jnp.bfloat16).astype(jnp.float32)
        rows_ref[2 * count * k : 2 * count * (k + 1), :] = part
        rest = rest - part
    rows_ref[6 * count : 7 * count, :] = silu(gathered(content_ref))
    rows_ref[7 * count : 8 * count, :] = gain_ref[...] * silu(gathered(outgate_ref))
    rows_ref[8 * count : 9 * count, :] = jnp.broadcast_to(strength * along, (count, wide))


def read_body(back_ref, rows_ref, readout_ref, sent_ref):
    wide = back_ref.shape[2]
    half = wide // 2
    count = back_ref.shape[0] // 2
    prompts = sent_ref.shape[1]
    heads = count // prompts
    pair = rows_ref[: 6 * count, :].astype(jnp.bfloat16)
    recalled, probed = [], []
    for n in range(count):
        state = jnp.concatenate([back_ref[2 * n, half:, :], back_ref[2 * n + 1, half:, :]], axis=0)
        found = lax.dot_general(
            pair, state, (((1,), (1,)), ((), ())), preferred_element_type=jnp.float32
        )
        found = found[: 2 * count] + found[2 * count : 4 * count] + found[4 * count :]
        recalled.append(found[n : n + 1])
        probed.append(found[count + n : count + n + 1])
    value, gate, weight = (rows_ref[k * count : (k + 1) * count, :] for k in (6, 7, 8))
    out = jnp.concatenate(probed, axis=0) + weight * (value - jnp.concatenate(recalled, axis=0))
    out = out * lax.rsqrt(jnp.mean(out * out, axis=-1, keepdims=True) + EPSILON)
    read = out * gate
    rows_of = [
        jnp.concatenate([read[p * heads + h :][:1] for h in range(heads)], axis=1)
        for p in range(prompts)
    ]
    heads_read = jnp.concatenate(rows_of, axis=0).astype(jnp.bfloat16)
    terms = jnp.dot(heads_read, readout_ref[...], preferred_element_type=jnp.float32)
    for k in range(sent_ref.shape[0]):
        sent_ref[k] = terms.astype(jnp.bfloat16)


SMEM = pl.BlockSpec(memory_space=pltpu.SMEM)


def local(body, name, shapes, *operands, kind=jnp.bfloat16, scalars=1):
    out = [jax.ShapeDtypeStruct(shape, kind) for shape in shapes]
    return pl.pallas_call(
        body,
        in_specs=[SMEM] * scalars + [VMEM] * (len(operands) - scalars),
        out_specs=[VMEM] * len(out),
        out_shape=out,
        interpret=INTERPRET,
        compiler_params=SMALL,
        name=name,
    )(*operands)


def per_device(
    tokens,
    address_projection,
    content_projection,
    strength_projection,
    fading_driver_projection,
    strength_offset,
    fading_speed,
    added_fading,
    probe,
    address,
    content,
    outgate,
    strength_raw,
    gain,
    readout_projection,
):
    prompts, positions, model = tokens.shape
    heads = fading_speed.shape[0]
    rows = prompts * positions
    share = model // (SIDE * SIDE)
    z, y, tp = lax.axis_index("z"), lax.axis_index("y"), lax.axis_index("tp")
    half = SIDE // 2
    my_half = y % 2

    weights = jnp.concatenate(
        [
            part[:, head * WIDTH : (head + 1) * WIDTH]
            for head in range(heads)
            for part in (address_projection, content_projection)
        ],
        axis=1,
    )
    flat = tokens.reshape(rows, model)
    columns = columns_by_owner(flat)
    line_tokens = exchange(columns, "y")
    line_weights = lax.all_gather(weights, "z", axis=0, tiled=True)

    drivers = jnp.concatenate([strength_projection, fading_driver_projection], axis=1)
    logits = jnp.dot(flat, drivers, preferred_element_type=jnp.float32).astype(jnp.bfloat16)
    logits = logits.astype(jnp.float32).reshape(prompts, positions, 2, -1)
    mine = lax.dynamic_slice_in_dim(logits, tp * heads, heads, 3)
    beta = jax.nn.sigmoid(mine[:, :, 0] + strength_offset)
    fading = added_fading - fading_speed * jax.nn.softplus(mine[:, :, 1])
    gates = jnp.stack([*two_parts(beta), *two_parts(fading)])
    gates = jnp.pad(
        gates.transpose(1, 3, 0, 2), ((0, 0), (0, 0), (0, 4), (0, 2 * WIDTH - positions))
    )

    gates = jnp.broadcast_to(gates[:, :, None], (prompts, heads, 2, *gates.shape[2:]))
    sent = partial_projections(
        line_tokens,
        line_weights,
        gates.reshape(prompts * heads, *gates.shape[2:]),
        positions,
    )
    got = exchange(sent.reshape(SIDE, *sent.shape[2:]), "y")

    side = my_half.astype(jnp.int32).reshape(1)
    size = (half * (WIDTH + WIDTH // 2), WIDTH)
    given, kept = local(ranges_body, "ranges", [size, size], side, got)
    other = lax.ppermute(given, "y", [(i, i ^ 1) for i in range(SIDE)])
    (line,) = local(line_body, "line", [(SIDE, WIDTH + WIDTH // 2, WIDTH)], side, kept, other)
    lines = exchange(line, "z")
    place = jnp.stack([z, my_half]).astype(jnp.int32)
    (home,) = local(scan_body, "scan", [(SIDE, WIDTH, WIDTH)], place, lines, kept, other)

    back = exchange(home, "y")
    (first_step,) = local(
        first_step_body,
        "first_step",
        [(9 * prompts * heads, WIDTH)],
        strength_raw,
        probe,
        address,
        content,
        outgate,
        gain.reshape(1, WIDTH),
        kind=jnp.float32,
    )
    sizes = [(lax.axis_size("tp"), prompts, readout_projection.shape[1])]
    (terms,) = local(read_body, "read", sizes, back, first_step, readout_projection, scalars=0)
    mixed = exchange(terms, "tp").astype(jnp.float32).sum(axis=0)
    states = back.reshape(prompts, heads, 2, 2, WIDTH // 2, WIDTH).transpose(3, 0, 1, 5, 2, 4)
    boundary, state_cache = states.reshape(2, prompts, heads, WIDTH, WIDTH)
    return state_cache, mixed.astype(jnp.bfloat16), boundary[:, None]


def solution(mesh):
    finer = Mesh(mesh.devices.reshape(SIDE, SIDE, mesh.shape["tp"]), (*SP, "tp"))
    return jax.shard_map(
        per_device,
        mesh=finer,
        in_specs=(
            P(None, SP, None),
            P(SP, "tp"),
            P(SP, "tp"),
            P(),
            P(),
            P("tp"),
            P("tp"),
            P(None, SP, "tp"),
            P(None, "tp"),
            P(None, "tp"),
            P(None, "tp"),
            P(None, "tp"),
            P(None, "tp"),
            P(),
            P("tp", SP),
        ),
        out_specs=(P(None, "tp", None, None), P(None, SP), P(None, SP, "tp", None, None)),
        check_vma=False,
    )
```

```python
import jax
import jax.numpy as jnp
from jax import lax
from jax.experimental import pallas as pl
from jax.experimental.pallas import tpu as pltpu
from jax.sharding import Mesh
from jax.sharding import PartitionSpec as P

WIDTH = 128
SIDE = 8
EPSILON = 1e-06
BEST = lax.Precision.HIGHEST
SP = ("z", "y")
INTERPRET = False
VMEM = pl.BlockSpec(memory_space=pltpu.VMEM)
SMALL = pltpu.CompilerParams(vmem_limit_bytes=16 * 1024 * 1024)


def exchange(messages, axis):
    return lax.all_to_all(messages, axis, split_axis=0, concat_axis=0, tiled=True)


def columns_body(tokens_ref, columns_ref, buffer_ref, arrived):
    parts, step, model = buffer_ref.shape
    share = model // (SIDE * SIDE)
    reads = [
        pltpu.make_async_copy(
            tokens_ref.at[i * step : (i + 1) * step, :], buffer_ref.at[i], arrived.at[i]
        )
        for i in range(parts)
    ]
    for read in reads:
        read.start()
    for i in range(parts):
        reads[i].wait()
        rows = buffer_ref[i]
        for to in range(SIDE):
            at = [(k * SIDE + to) * share for k in range(SIDE)]
            columns_ref[to, i * step : (i + 1) * step, :] = jnp.concatenate(
                [rows[:, a : a + share] for a in at], axis=1
            )


def columns_by_owner(flat, parts=4):
    rows, model = flat.shape
    return pl.pallas_call(
        columns_body,
        in_specs=[pl.BlockSpec(memory_space=pltpu.MemorySpace.HBM)],
        out_specs=VMEM,
        out_shape=jax.ShapeDtypeStruct((SIDE, rows, model // SIDE), flat.dtype),
        scratch_shapes=[
            pltpu.VMEM((parts, rows // parts, model), flat.dtype),
            pltpu.SemaphoreType.DMA((parts,)),
        ],
        interpret=INTERPRET,
        name="columns",
    )(flat)


def partial_body(tokens_ref, weights_ref, gates_ref, out_ref, sent_ref, done):
    line, rows, _ = tokens_ref.shape
    owners, halves, sent_rows, width = sent_ref.shape
    ranges = line // halves
    positions = (sent_rows - gates_ref.shape[2]) // ranges
    prompts = rows // positions
    heads = owners // prompts
    sent_ref[:, :, ranges * positions :, :] = gates_ref[...]
    writes = [
        pltpu.make_async_copy(sent_ref.at[:, half], out_ref.at[:, half], done.at[half])
        for half in range(halves)
    ]
    for k in range(line):
        half, j = k // ranges, k % ranges
        part = jnp.dot(tokens_ref[k], weights_ref[...], preferred_element_type=jnp.float32)
        part = part.astype(sent_ref.dtype)
        for p in range(prompts):
            for h in range(heads):
                sent_ref[p * heads + h, half, j * positions : (j + 1) * positions, :] = part[
                    p * positions : (p + 1) * positions, h * width : (h + 1) * width
                ]
        if j == ranges - 1:
            writes[half].start()
    for write in writes:
        write.wait()


def partial_projections(tokens, weights, gates, positions):
    owners, halves, extra, width = gates.shape
    shape = (owners, halves, tokens.shape[0] // halves * positions + extra, width)
    return pl.pallas_call(
        partial_body,
        in_specs=[VMEM, VMEM, VMEM],
        out_specs=pl.BlockSpec(memory_space=pltpu.MemorySpace.HBM),
        out_shape=jax.ShapeDtypeStruct(shape, tokens.dtype),
        scratch_shapes=[pltpu.VMEM(shape, tokens.dtype), pltpu.SemaphoreType.DMA((halves,))],
        interpret=INTERPRET,
        compiler_params=SMALL,
        name="partials",
    )(tokens, weights, gates)


def two_parts(values):
    high = lax.reduce_precision(values, 8, 7)
    return high.astype(jnp.bfloat16), (values - high).astype(jnp.bfloat16)


def best(left, right, dims=((1,), (0,))):
    return lax.dot_general(
        left, right, (dims, ((), ())), precision=BEST, preferred_element_type=jnp.float32
    )


def parts(x):
    high = x.astype(jnp.bfloat16)
    return high, (x - high.astype(jnp.float32)).astype(jnp.bfloat16)


def times(state, matrix):
    rows = state.shape[0]
    both = jnp.dot(
        jnp.concatenate(parts(state), axis=0), matrix, preferred_element_type=jnp.float32
    )
    return both[:rows] + both[rows:]


def near(left, right, dims=((1,), (0,))):
    (a, b), (c, d) = parts(left), parts(right)

    def dot(u, v):
        return lax.dot_general(u, v, (dims, ((), ())), preferred_element_type=jnp.float32)

    return dot(a, c) + (dot(a, d) + dot(b, c))


def silu(x):
    return x / (1.0 + jnp.exp(-x))


def ranges_body(half_ref, got_ref, sent_ref, kept_ref):
    line, _, width = got_ref.shape
    wide = width // 2
    ranges = line // 2
    positions = sent_ref.shape[0] // (ranges * 3)
    count = ranges * positions
    half = half_ref[0]
    sums = got_ref[0, :count, :].astype(jnp.float32)
    for k in range(1, line):
        sums = sums + got_ref[k, :count, :].astype(jnp.float32)
    keys = silu(sums[:, :wide])
    keys = keys * lax.rsqrt(jnp.sum(keys * keys, axis=-1, keepdims=True) + EPSILON)
    values = silu(sums[:, wide:])
    gates = got_ref[pl.ds(half * ranges, ranges), count:, :wide].astype(jnp.float32)
    beta = gates[:, 0, :] + gates[:, 1, :]
    fading = gates[:, 2, :] + gates[:, 3, :]
    up_to = lax.broadcasted_iota(jnp.int32, (wide, wide), 0) <= lax.broadcasted_iota(
        jnp.int32, (wide, wide), 1
    )
    sums_to = best(jnp.concatenate([beta, fading], axis=0), up_to.astype(jnp.float32))[ranges:]
    columns = jnp.concatenate([beta, sums_to], axis=0).T
    row = lax.broadcasted_iota(jnp.int32, (positions, positions), 0)
    column = lax.broadcasted_iota(jnp.int32, (positions, positions), 1)
    strict = row > column
    unit = (
        lax.broadcasted_iota(jnp.int32, (wide, wide), 0)
        == lax.broadcasted_iota(jnp.int32, (wide, wide), 1)
    ).astype(jnp.float32)
    powers, solved, tails, lasts = [], [], [], []
    for j in range(ranges):
        at = slice(j * positions, (j + 1) * positions)
        b = columns[:positions, j : j + 1]
        total = columns[:positions, ranges + j : ranges + j + 1]
        last = total[positions - 1 :, :]
        across = sums_to[j : j + 1, :positions]
        scaled = keys[at] * b
        inner = best(scaled, keys[at], ((1,), (1,)))
        spread = jnp.exp(jnp.where(strict, total - across, 0.0))
        powers.append(jnp.where(strict, inner * spread, 0.0))
        solved.append(jnp.concatenate([scaled * jnp.exp(total), values[at] * b], axis=1))
        tails.append(keys[at] * jnp.exp(last - total))
        lasts.append(jnp.exp(last))
    for j in range(ranges):
        solved[j] = solved[j] - best(powers[j], solved[j])
    reached = 2
    while reached < positions:
        for j in range(ranges):
            powers[j] = best(powers[j], powers[j])
        for j in range(ranges):
            solved[j] = solved[j] + best(powers[j], solved[j])
        reached *= 2
    so_far = None
    for j in range(ranges):
        moved = near(solved[j], tails[j], ((0,), (0,)))
        step = lasts[j] * unit - moved[:wide]
        if so_far is None:
            so_far = jnp.concatenate([step, moved[wide:]], axis=0)
        else:
            both = near(so_far, step)
            so_far = jnp.concatenate([both[:wide], both[wide:] + moved[wide:]], axis=0)
        out = so_far.astype(jnp.bfloat16)
        low, high = out[wide : wide + positions], out[wide + positions :]
        sent_ref[j * wide : (j + 1) * wide, :] = out[:wide]
        at = slice(ranges * wide + j * positions, ranges * wide + (j + 1) * positions)
        sent_ref[at, :] = jnp.where(half == 0, high, low)
        kept_ref[j * wide : (j + 1) * wide, :] = out[:wide]
        kept_ref[at, :] = jnp.where(half == 0, low, high)


def line_body(half_ref, kept_ref, other_ref, sent_ref):
    count, wide = kept_ref.shape
    ranges = 2 * count // (3 * wide)
    rows = wide // 2
    mine_first = half_ref[0] == 0
    step = slice((ranges - 1) * wide, ranges * wide)
    kept = jnp.concatenate([kept_ref[step, :], kept_ref[count - rows :, :]], axis=0)
    other = jnp.concatenate([other_ref[step, :], other_ref[count - rows :, :]], axis=0)
    first = jnp.where(mine_first, kept, other)
    second = jnp.where(mine_first, other, kept)
    both = jnp.dot(first, second[:wide], preferred_element_type=jnp.float32)
    added = both[wide:] + second[wide:].astype(jnp.float32)
    out = jnp.concatenate([both[:wide], added], axis=0).astype(jnp.bfloat16)
    for k in range(sent_ref.shape[0]):
        sent_ref[k] = out


def scan_body(place_ref, lines_ref, kept_ref, other_ref, sent_ref):
    lines, _, wide = lines_ref.shape
    rows = wide // 2
    ranges = sent_ref.shape[0] // 2
    z, mine_first = place_ref[0], place_ref[1] == 0
    after, pairs = [], []
    for k in range(0, lines, 2):
        both = jnp.dot(
            lines_ref[k], lines_ref[k + 1, :wide, :], preferred_element_type=jnp.float32
        )
        added = both[wide:] + lines_ref[k + 1, wide:, :].astype(jnp.float32)
        pairs.append((parts(both[:wide]), added))
    state = jnp.zeros((rows, wide), jnp.float32)
    for k, ((high, low), added) in enumerate(pairs):
        after.append(state)
        if k:
            ours = jnp.concatenate(parts(state), axis=0)
            found = jnp.dot(ours, high, preferred_element_type=jnp.float32)
            found = found[:rows] + found[rows:]
            state = found + jnp.dot(ours[:rows], low, preferred_element_type=jnp.float32) + added
        else:
            state = added
    begin = after[0]
    for k in range(1, len(after)):
        begin = jnp.where(z // 2 == k, after[k], begin)
    before = lines_ref[(z // 2) * 2]
    stepped = times(begin, before[:wide]) + before[wide:].astype(jnp.float32)
    entering = jnp.where(z % 2 == 0, begin, stepped)
    final = state.astype(jnp.bfloat16)
    state = entering
    for h in range(2):
        begin = state
        for j in range(ranges):
            step = slice(j * wide, (j + 1) * wide)
            extra = slice(ranges * wide + j * rows, ranges * wide + (j + 1) * rows)
            use_kept = mine_first if h == 0 else jnp.logical_not(mine_first)
            matrix = jnp.where(use_kept, kept_ref[step, :], other_ref[step, :])
            added = jnp.where(use_kept, kept_ref[extra, :], other_ref[extra, :])
            state = times(begin, matrix) + added.astype(jnp.float32)
            sent_ref[h * ranges + j, :rows, :] = state.astype(jnp.bfloat16)
            sent_ref[h * ranges + j, rows:, :] = final


def first_step_body(
    strength_ref, probe_ref, address_ref, content_ref, outgate_ref, gain_ref, rows_ref
):
    prompts, width = probe_ref.shape
    wide = gain_ref.shape[1]
    each = [(p, h) for p in range(prompts) for h in range(width // wide)]
    count = len(each)

    def gathered(ref):
        wanted = [ref[p : p + 1, h * wide : (h + 1) * wide] for p, h in each]
        return jnp.concatenate(wanted, axis=0).astype(jnp.float32)

    query = silu(gathered(probe_ref))
    key = silu(gathered(address_ref))
    key = key * lax.rsqrt(jnp.sum(key * key, axis=-1, keepdims=True) + EPSILON)
    strength = jnp.concatenate(
        [jnp.full((1, 1), strength_ref[p, h], jnp.float32) for p, h in each], axis=0
    )
    strength = 1.0 / (1.0 + jnp.exp(-strength))
    along = jnp.sum(key * query, axis=-1, keepdims=True)
    rest = jnp.concatenate([key, query], axis=0)
    for k in range(3):
        part = rest.astype(jnp.bfloat16).astype(jnp.float32)
        rows_ref[2 * count * k : 2 * count * (k + 1), :] = part
        rest = rest - part
    rows_ref[6 * count : 7 * count, :] = silu(gathered(content_ref))
    rows_ref[7 * count : 8 * count, :] = gain_ref[...] * silu(gathered(outgate_ref))
    rows_ref[8 * count : 9 * count, :] = jnp.broadcast_to(strength * along, (count, wide))


def read_body(back_ref, rows_ref, readout_ref, sent_ref):
    wide = back_ref.shape[2]
    half = wide // 2
    count = back_ref.shape[0] // 2
    prompts = sent_ref.shape[1]
    heads = count // prompts
    pair = rows_ref[: 6 * count, :].astype(jnp.bfloat16)
    recalled, probed = [], []
    for n in range(count):
        state = jnp.concatenate([back_ref[2 * n, half:, :], back_ref[2 * n + 1, half:, :]], axis=0)
        found = lax.dot_general(
            pair, state, (((1,), (1,)), ((), ())), preferred_element_type=jnp.float32
        )
        found = found[: 2 * count] + found[2 * count : 4 * count] + found[4 * count :]
        recalled.append(found[n : n + 1])
        probed.append(found[count + n : count + n + 1])
    value, gate, weight = (rows_ref[k * count : (k + 1) * count, :] for k in (6, 7, 8))
    out = jnp.concatenate(probed, axis=0) + weight * (value - jnp.concatenate(recalled, axis=0))
    out = out * lax.rsqrt(jnp.mean(out * out, axis=-1, keepdims=True) + EPSILON)
    read = out * gate
    rows_of = [
        jnp.concatenate([read[p * heads + h :][:1] for h in range(heads)], axis=1)
        for p in range(prompts)
    ]
    heads_read = jnp.concatenate(rows_of, axis=0).astype(jnp.bfloat16)
    terms = jnp.dot(heads_read, readout_ref[...], preferred_element_type=jnp.float32)
    for k in range(sent_ref.shape[0]):
        sent_ref[k] = terms.astype(jnp.bfloat16)


SMEM = pl.BlockSpec(memory_space=pltpu.SMEM)


def local(body, name, shapes, *operands, kind=jnp.bfloat16, scalars=1):
    out = [jax.ShapeDtypeStruct(shape, kind) for shape in shapes]
    return pl.pallas_call(
        body,
        in_specs=[SMEM] * scalars + [VMEM] * (len(operands) - scalars),
        out_specs=[VMEM] * len(out),
        out_shape=out,
        interpret=INTERPRET,
        compiler_params=SMALL,
        name=name,
    )(*operands)


def per_device(
    tokens,
    address_projection,
    content_projection,
    strength_projection,
    fading_driver_projection,
    strength_offset,
    fading_speed,
    added_fading,
    probe,
    address,
    content,
    outgate,
    strength_raw,
    gain,
    readout_projection,
):
    prompts, positions, model = tokens.shape
    heads = fading_speed.shape[0]
    rows = prompts * positions
    share = model // (SIDE * SIDE)
    z, y, tp = lax.axis_index("z"), lax.axis_index("y"), lax.axis_index("tp")
    half = SIDE // 2
    my_half = y % 2

    weights = jnp.concatenate(
        [
            part[:, head * WIDTH : (head + 1) * WIDTH]
            for head in range(heads)
            for part in (address_projection, content_projection)
        ],
        axis=1,
    )
    flat = tokens.reshape(rows, model)
    columns = columns_by_owner(flat)
    line_tokens = exchange(columns, "y")
    line_weights = lax.all_gather(weights, "z", axis=0, tiled=True)

    drivers = jnp.concatenate([strength_projection, fading_driver_projection], axis=1)
    logits = jnp.dot(flat, drivers, preferred_element_type=jnp.float32).astype(jnp.bfloat16)
    logits = logits.astype(jnp.float32).reshape(prompts, positions, 2, -1)
    mine = lax.dynamic_slice_in_dim(logits, tp * heads, heads, 3)
    beta = jax.nn.sigmoid(mine[:, :, 0] + strength_offset)
    fading = added_fading - fading_speed * jax.nn.softplus(mine[:, :, 1])
    gates = jnp.stack([*two_parts(beta), *two_parts(fading)])
    gates = jnp.pad(
        gates.transpose(1, 3, 0, 2), ((0, 0), (0, 0), (0, 4), (0, 2 * WIDTH - positions))
    )

    gates = jnp.broadcast_to(gates[:, :, None], (prompts, heads, 2, *gates.shape[2:]))
    sent = partial_projections(
        line_tokens,
        line_weights,
        gates.reshape(prompts * heads, *gates.shape[2:]),
        positions,
    )
    got = exchange(sent.reshape(SIDE, *sent.shape[2:]), "y")

    side = my_half.astype(jnp.int32).reshape(1)
    size = (half * (WIDTH + WIDTH // 2), WIDTH)
    given, kept = local(ranges_body, "ranges", [size, size], side, got)
    other = lax.ppermute(given, "y", [(i, i ^ 1) for i in range(SIDE)])
    (line,) = local(line_body, "line", [(SIDE, WIDTH + WIDTH // 2, WIDTH)], side, kept, other)
    lines = exchange(line, "z")
    place = jnp.stack([z, my_half]).astype(jnp.int32)
    (home,) = local(scan_body, "scan", [(SIDE, WIDTH, WIDTH)], place, lines, kept, other)

    back = exchange(home, "y")
    (first_step,) = local(
        first_step_body,
        "first_step",
        [(9 * prompts * heads, WIDTH)],
        strength_raw,
        probe,
        address,
        content,
        outgate,
        gain.reshape(1, WIDTH),
        kind=jnp.float32,
    )
    sizes = [(lax.axis_size("tp"), prompts, readout_projection.shape[1])]
    (terms,) = local(read_body, "read", sizes, back, first_step, readout_projection, scalars=0)
    mixed = exchange(terms, "tp").astype(jnp.float32).sum(axis=0)
    states = back.reshape(prompts, heads, 2, 2, WIDTH // 2, WIDTH).transpose(3, 0, 1, 5, 2, 4)
    boundary, state_cache = states.reshape(2, prompts, heads, WIDTH, WIDTH)
    return state_cache, mixed.astype(jnp.bfloat16), boundary[:, None]


def solution(mesh):
    finer = Mesh(mesh.devices.reshape(SIDE, SIDE, mesh.shape["tp"]), (*SP, "tp"))
    return jax.shard_map(
        per_device,
        mesh=finer,
        in_specs=(
            P(None, SP, None),
            P(SP, "tp"),
            P(SP, "tp"),
            P(),
            P(),
            P("tp"),
            P("tp"),
            P(None, SP, "tp"),
            P(None, "tp"),
            P(None, "tp"),
            P(None, "tp"),
            P(None, "tp"),
            P(None, "tp"),
            P(),
            P("tp", SP),
        ),
        out_specs=(P(None, "tp", None, None), P(None, SP), P(None, SP, "tp", None, None)),
        check_vma=False,
    )
```
